32 devices in a mesh: ep: 8 (over z, x), tp: 4 (over y, core).
Axes of the slice: x: 2, y: 2, z: 4, core: 2. Of those that a mesh axis runs over, the one named last changes fastest.
Arguments:
- queries: bfloat16 [2048, 1536], P('ep', 'tp'), may hold values from -600 to 600
- compressed_key_value: bfloat16 [2048, 512], P('ep'), may hold values from -6 to 6
- rope_key: bfloat16 [2048, 32], P('ep'), may hold values from -6 to 6
- latent_norm_gain: float32 [512], replicated, may hold values from 0.1 to 1.9
- latent_to_key_value: bfloat16 [512, 2048], P(None, 'tp'), may hold values from -0.25 to 0.25
- out_proj: bfloat16 [1024, 2048], P(None, 'tp'), may hold values from -1.5 to 1.5
- moe_input: bfloat16 [2048, 2048], P('ep'), may hold values from -6 to 6
- moe_gain: float32 [2048], replicated, may hold values from 0.1 to 1.9
- routes: int32 [2048, 2], P('ep'), may hold values from 0 to 7, all different within a row; in each aligned block of 256 rows (0 to 255, 256 to 511, ...) at most 96 rows name the same one
- route_weight: float32 [2048, 2], P('ep'), may hold values from 0.2 to 1
- gate_weight: bfloat16 [8, 2048, 4096], P('ep', None, 'tp'), may hold values from -0.125 to 0.125
- up_weight: bfloat16 [8, 2048, 4096], P('ep', None, 'tp'), may hold values from -0.125 to 0.125
- down_weight: bfloat16 [8, 4096, 2048], P('ep', 'tp'), may hold values from -0.09375 to 0.09375
Outputs:
- attention_out: bfloat16 [2048, 2048], P('ep', 'tp')
- expert_out: bfloat16 [2048, 2048], P('ep', 'tp')
The draws below stay inside these ranges and needn't reach their ends.
Inputs may be any that keep to these rules, and one draw needn't show every extreme that they name: `routes`: each row names 2 different experts. In the rows of one device (aligned blocks of 256 rows) no expert is named by more than 96 rows, and in some blocks one expert is named by exactly 96 rows.
All inputs are finite; a program needn't handle non-finite values.
Results may differ from the reference program's by a relative error of at most 0.019.
The reference program's roundings to bfloat16 on the way count: a program that leaves them out, or rounds other values in their place, can miss the bound.
Values may be sent and summed in bfloat16 or wider, within the bound.
A program may use at most 128 MiB of HBM per device.

```python
import math
import jax
import jax.numpy as jnp
import numpy as np
from jax import lax

D = 2048
ATTENTION_HEADS = 16
PLAIN_HEAD_DIM = 64
ROPE = 32
VALUE_HEAD_DIM = 64
LATENT_WIDTH = 512
EXPERT_FF = 4096
TOP = 2
TOK_DEV = 256
MLA_W = 1024
MICRO_TOKENS = 2048
EXPERTS = 8
CAP = 96
N_EP = 8
N_TP = 4


def draw_queries(key, part):
    base_values = jax.random.normal(key, (MICRO_TOKENS, ATTENTION_HEADS * (PLAIN_HEAD_DIM + ROPE)), jnp.float32) * 2.0
    return jnp.clip(base_values, -600.0, 600.0).astype(jnp.bfloat16)


def block_scale(rng, shape, split, low, largest):
    factor_of, own = 1.0, jax.random.fold_in(rng, 6)
    for dim, shards_of in split:
        heights = jnp.exp(jax.random.uniform(jax.random.fold_in(own, dim), (shards_of,), jnp.float32, low / len(split), largest / len(split)))
        factor_of = factor_of * jnp.repeat(heights, shape[dim] // shards_of).reshape([-1 if axis == dim else 1 for axis in range(len(shape))])
    return factor_of


def assign_block(rng, own, number, rows, number_of, top, limit, skew):
    sequence = jax.random.permutation(rng, number_of)
    crowded, usual = shares(number_of, rows * top, limit, skew, True), shares(number_of, rows * top, limit, skew, False)
    places = jnp.arange(number_of)

    def named(sizes, offset_by):
        used = int((sizes > 0).sum())
        fixed = max(1, used // 4)
        shifted = fixed + (places - fixed + offset_by * (used - fixed)) % max(1, number_of - fixed)
        return jnp.zeros((number_of,), jnp.int32).at[sequence[jnp.where(places < fixed, places, shifted)]].set(jnp.asarray(sizes, jnp.int32))

    sizes = jnp.where(number % 4 == 0, named(crowded, number // 4), named(usual, number - number // 4 - 1))
    mixed = jax.random.permutation(jax.random.fold_in(own, 3), number_of)
    source_of, receiver = mixed[0:number_of // 2 * 2:2], mixed[1:number_of // 2 * 2:2]
    room = jnp.minimum(sizes[source_of] - 1, limit - sizes[receiver]) // 2
    room = jnp.where((source_of == sequence[0]) | (receiver == sequence[0]) | (sizes[receiver] == 0), 0, jnp.maximum(room, 0))
    shifted = jax.random.randint(jax.random.fold_in(own, 4), (number_of // 2,), 0, 1 << 20) % (room + 1)
    sizes = sizes.at[source_of].add(-shifted).at[receiver].add(shifted)
    members = jnp.searchsorted(jnp.cumsum(sizes), jnp.arange(rows * top), side="right").astype(jnp.int32)
    table = members.reshape(top, rows).T
    table = table[jax.random.permutation(jax.random.fold_in(own, 1), rows)]
    offset_by = jax.random.randint(jax.random.fold_in(own, 2), (rows, 1), 0, top)
    return jnp.take_along_axis(table, (jnp.arange(top)[None, :] + offset_by) % top, axis=1)


def shares(number_of, total, bound, skew, full):
    portions = [(1 << 20) // math.isqrt(standing ** skew) + 1 for standing in range(1, number_of + 1)]
    largest = bound if full else min(bound, max(-(-total // number_of), total * portions[0] // sum(portions)))
    least = 1 if total - largest >= number_of - 1 else 0
    given, spare = [largest] + [least] * (number_of - 1), total - largest - least * (number_of - 1)
    while spare > 0:
        free = [i for i in range(1, number_of) if given[i] < largest] or [i for i in range(1, number_of) if given[i] < bound]
        mass, remaining = sum([portions[i] for i in free]), spare
        for i in free:
            extra = min(bound - given[i], max(1, remaining * portions[i] // mass), spare)
            given[i] = given[i] + extra
            spare = spare - extra
    return np.array(given)


def bell_draw(stream_key, extent, deviation, limit, pieces=(), held_as=jnp.bfloat16):
    drawn = jax.random.normal(stream_key, extent, jnp.float32) * deviation
    if len(pieces) > 0:
        drawn = block_scale(stream_key, extent, pieces, -0.22, 0.18) * drawn
    return jnp.clip(drawn, min=-limit, max=limit).astype(held_as)


def setup_inputs(seed: int = 0) -> dict:
    key_list = jax.random.split(jax.random.key(seed), 14)
    queries = draw_queries(jax.random.fold_in(key_list[13], 71), 0)
    compressed_key_value = bell_draw(key_list[1], (MICRO_TOKENS, LATENT_WIDTH), 1.0, 6.0, ((0, 8),))
    rope_key = bell_draw(key_list[2], (MICRO_TOKENS, ROPE), 1.0, 6.0, ((0, 8),))
    latent_norm_gain = jnp.clip(1.0 + 0.18 * jax.random.normal(key_list[3], (LATENT_WIDTH,), jnp.float32), 0.1, 1.9)
    latent_to_key_value = bell_draw(key_list[4], (LATENT_WIDTH, ATTENTION_HEADS * (PLAIN_HEAD_DIM + VALUE_HEAD_DIM)), LATENT_WIDTH ** -0.5, 0.25, ((1, 4),))
    out_proj = bell_draw(key_list[5], (MLA_W, D), ATTENTION_HEADS ** -0.5, 1.5, ((1, 4),))
    moe_input = bell_draw(key_list[6], (MICRO_TOKENS, D), 1.0, 6.0, ((0, 8),))
    moe_gain = jnp.clip(1.0 + 0.18 * jax.random.normal(key_list[7], (D,), jnp.float32), 0.1, 1.9)
    routes_keys = jax.random.split(jax.random.fold_in(key_list[8], 1), MICRO_TOKENS // TOK_DEV)
    routes_turns = jax.random.permutation(jax.random.fold_in(key_list[8], 3), MICRO_TOKENS // TOK_DEV)
    routes = jax.vmap(lambda own, number: assign_block(jax.random.fold_in(key_list[8], 2), own, number, TOK_DEV, EXPERTS, TOP, CAP, 2))(routes_keys, routes_turns).reshape((MICRO_TOKENS, TOP))
    route_weight = jnp.clip(0.2 + 0.8 * jax.random.uniform(key_list[9], (MICRO_TOKENS, TOP), jnp.float32) ** block_scale(key_list[9], (MICRO_TOKENS, TOP), ((0, 8),), -0.2, 0.2), 0.2, 1.0)
    gate_weight = bell_draw(key_list[10], (EXPERTS, D, EXPERT_FF), D ** -0.5, 0.125, ((0, 8), (2, 4)))
    up_weight = bell_draw(key_list[11], (EXPERTS, D, EXPERT_FF), D ** -0.5, 0.125, ((0, 8), (2, 4)))
    down_weight = bell_draw(key_list[12], (EXPERTS, EXPERT_FF, D), EXPERT_FF ** -0.5, 0.09375, ((0, 8), (1, 4)))
    return {"queries": queries, "compressed_key_value": compressed_key_value, "rope_key": rope_key, "latent_norm_gain": latent_norm_gain, "latent_to_key_value": latent_to_key_value, "out_proj": out_proj, "moe_input": moe_input, "moe_gain": moe_gain, "routes": routes, "route_weight": route_weight, "gate_weight": gate_weight, "up_weight": up_weight, "down_weight": down_weight}


EPSILON = 1e-06
ROPE_BASE_VALUE = 10000.0

def rms_scale(values, gain_vector):
    floats = values.astype(jnp.float32)
    return floats * lax.rsqrt(lax.optimization_barrier(jnp.mean(floats * floats, axis=-1, keepdims=True)) + EPSILON) * gain_vector.astype(jnp.float32)

def rotary(values, positions):
    full_width = values.shape[-1]
    half_dim = full_width // 2
    frequency = ROPE_BASE_VALUE ** (-jnp.arange(half_dim, dtype=jnp.float32) * 2.0 / full_width)
    angles = positions[..., None] * frequency
    cosine = jnp.cos(angles)
    sine_part = jnp.sin(angles)
    first_half = values[..., :half_dim]
    second_half = values[..., half_dim:]
    return jnp.concatenate([first_half * cosine - second_half * sine_part, second_half * cosine + first_half * sine_part], axis=-1)

def slot_table(block_routes, capacity, experts):
    flat_routes = block_routes.reshape(-1).astype(jnp.int32)
    onehot_table = (flat_routes[:, None] == jnp.arange(experts, dtype=jnp.int32)[None, :]).astype(jnp.int32)
    earlier = jnp.cumsum(onehot_table, axis=0) - onehot_table
    slot_index = lax.optimization_barrier(jnp.sum(earlier * onehot_table, axis=1)).astype(jnp.int32)
    destination = (flat_routes * capacity + slot_index).astype(jnp.int32)
    token_count = block_routes.shape[0]
    source_rows = (jnp.arange(flat_routes.shape[0], dtype=jnp.int32) // block_routes.shape[1]).astype(jnp.int32)
    source_table = jnp.full((experts * capacity,), token_count, jnp.int32).at[destination].set(source_rows)
    return (destination, source_table)

def reference(queries, compressed_key_value, rope_key, latent_norm_gain, latent_to_key_value, out_proj, moe_input, moe_gain, routes, route_weight, gate_weight, up_weight, down_weight):
    positions = jnp.arange(MICRO_TOKENS, dtype=jnp.float32)
    query_heads = queries.reshape(MICRO_TOKENS, ATTENTION_HEADS, PLAIN_HEAD_DIM + ROPE)
    query_nope = query_heads[..., :PLAIN_HEAD_DIM]
    query_rope = rotary(query_heads[..., PLAIN_HEAD_DIM:].astype(jnp.float32), positions[:, None]).astype(jnp.bfloat16)
    latent_normed = rms_scale(compressed_key_value, latent_norm_gain).astype(jnp.bfloat16)
    key_value = jnp.dot(latent_normed, latent_to_key_value, preferred_element_type=jnp.float32).astype(jnp.bfloat16)
    key_value = key_value.reshape(MICRO_TOKENS, ATTENTION_HEADS, PLAIN_HEAD_DIM + VALUE_HEAD_DIM)
    key_rope = rotary(rope_key.astype(jnp.float32), positions).astype(jnp.bfloat16)
    score_scale = (PLAIN_HEAD_DIM + ROPE) ** (-0.5)

    def one_head(inputs):
        head_nope, head_rope, head_kv = inputs
        key_nope = head_kv[:, :PLAIN_HEAD_DIM]
        head_values = head_kv[:, PLAIN_HEAD_DIM:]

        def one_block(block_inputs):
            block_nope, block_rope = block_inputs
            scores = (jnp.dot(block_nope, key_nope.T, preferred_element_type=jnp.float32) + jnp.dot(block_rope, key_rope.T, preferred_element_type=jnp.float32)) * score_scale
            row_max = lax.optimization_barrier(jnp.max(scores, axis=-1, keepdims=True))
            weights = jnp.exp(scores - row_max)
            row_total = lax.optimization_barrier(jnp.sum(weights, axis=-1, keepdims=True))
            mixed_rows = jnp.dot(weights.astype(jnp.bfloat16), head_values, preferred_element_type=jnp.float32) / row_total
            return mixed_rows.astype(jnp.bfloat16)
        blocks_out = lax.map(one_block, (head_nope.reshape(N_EP, TOK_DEV, PLAIN_HEAD_DIM), head_rope.reshape(N_EP, TOK_DEV, ROPE)))
        return blocks_out.reshape(MICRO_TOKENS, VALUE_HEAD_DIM)
    per_head = lax.map(one_head, (query_nope.transpose(1, 0, 2), query_rope.transpose(1, 0, 2), key_value.transpose(1, 0, 2)))
    attended = per_head.transpose(1, 0, 2).reshape(MICRO_TOKENS, ATTENTION_HEADS * VALUE_HEAD_DIM)
    attention_out = jnp.dot(attended, out_proj, preferred_element_type=jnp.float32).astype(jnp.bfloat16)
    normed = rms_scale(moe_input, moe_gain).astype(jnp.bfloat16)
    destination, source_table = jax.vmap(lambda block_routes: slot_table(block_routes, CAP, EXPERTS))(routes.reshape(N_EP, TOK_DEV, TOP))
    padded = jnp.concatenate([normed.reshape(N_EP, TOK_DEV, D), jnp.zeros((N_EP, 1, D), jnp.bfloat16)], axis=1)
    outgoing = jax.vmap(lambda table_rows, row_index: table_rows[row_index])(padded, source_table)
    per_expert = outgoing.reshape(N_EP, EXPERTS, CAP, D).transpose(1, 0, 2, 3).reshape(EXPERTS, N_EP * CAP, D)
    width_block = EXPERT_FF // N_TP

    def one_expert(inputs):
        expert_rows, gate_matrix, up_matrix, down_matrix = inputs
        gate_value = jnp.dot(expert_rows, gate_matrix, preferred_element_type=jnp.float32)
        up_value = jnp.dot(expert_rows, up_matrix, preferred_element_type=jnp.float32)
        hidden = (jax.nn.silu(gate_value) * up_value).astype(jnp.bfloat16)
        partial_sums = jnp.einsum('rjf,jfd->jrd', hidden.reshape(-1, N_TP, width_block).astype(jnp.float32), down_matrix.reshape(N_TP, width_block, D).astype(jnp.float32))
        rounded = lax.optimization_barrier(partial_sums.astype(jnp.bfloat16))
        return lax.optimization_barrier(jnp.sum(rounded.astype(jnp.float32), axis=0)).astype(jnp.bfloat16)
    results = lax.map(one_expert, (per_expert, gate_weight, up_weight, down_weight))
    returned = results.reshape(EXPERTS, N_EP, CAP, D).transpose(1, 0, 2, 3).reshape(N_EP, EXPERTS * CAP, D)
    picked = jax.vmap(lambda table_rows, row_index: table_rows[row_index])(returned, destination)
    weighted = picked.astype(jnp.float32).reshape(N_EP, TOK_DEV, TOP, D) * route_weight.reshape(N_EP, TOK_DEV, TOP, 1)
    expert_out = lax.optimization_barrier(jnp.sum(weighted, axis=2)).reshape(MICRO_TOKENS, D).astype(jnp.bfloat16)
    return (attention_out, expert_out)
```

```python
import functools

import jax
import jax.numpy as jnp
import numpy as np
from jax import lax
from jax.experimental import pallas as pl
from jax.experimental.pallas import tpu as pltpu
from jax.sharding import PartitionSpec as P

PLAIN_HEAD_DIM = 64
ROPE = 32
VALUE_HEAD_DIM = 64
LANES = 128
CORES = 2


EPSILON = 1e-06
ROPE_BASE_VALUE = 10000.0


def ep_shape(n_ep):
    nx = 2 if n_ep % 2 == 0 else 1
    return nx, n_ep // nx


def partners(nz):
    side = lambda z: 2 * z < nz
    return [
        sorted(
            (o for o in range(nz) if o != z),
            key=lambda o: (abs(o - z), side(o) != side(z), o),
        )
        for z in range(nz)
    ]


def merge_rows(block):
    return block.reshape(block.shape[0] * block.shape[1], block.shape[2])


def fused(
    n_ep,
    n_tp,
    heads,
    scale,
    routes_ref,
    weight_ref,
    mgain_ref,
    lgain_ref,
    rope_ref,
    moe_hbm,
    ckv_hbm,
    q_hbm,
    wkv_hbm,
    wo_hbm,
    wg_hbm,
    wu_hbm,
    wd_hbm,
    att_out,
    exp_out,
    moe_v,
    ckv_v,
    qraw,
    wkv_ref,
    wo_ref,
    wg,
    wu,
    wd,
    normed,
    key_ref,
    mix_ref,
    out_z,
    out_x,
    rope_v,
    q_ref,
    g_lat,
    g_moe,
    g_att,
    kv,
    hidden,
    part,
    r1,
    s2,
    r2,
    tot,
    back,
    in_sem,
    lat_up,
    lat_dn,
    lat_x,
    lat_c,
    moe_a,
    moe_x,
    moe_xc,
    moe_y,
    moe_c,
    att_y,
    att_c,
    red_c,
    red_y,
    ret_a,
):
    f32, bf16 = jnp.float32, jnp.bfloat16
    frequency_of = ROPE_BASE_VALUE ** (-np.arange(ROPE // 2, dtype=np.float32) * 2.0 / ROPE)
    me = lax.axis_index("ep")
    tp = lax.axis_index("tp")
    n_y = n_tp // CORES
    my_y = tp // CORES
    my_c = lax.rem(tp, CORES)
    mate = my_y * CORES + (1 - my_c)
    nx, nz = ep_shape(n_ep)
    my_z = me // nx
    my_x = lax.rem(me, nx)
    row_count, model_width = moe_v.shape
    columns = model_width // n_tp
    cap = g_moe.shape[2]
    chunks = nz
    rows = nx * cap
    ff = wg.shape[1]
    tile = min(256, ff)
    tiles = ff // tile
    share = ckv_v.shape[0]
    latent = ckv_v.shape[1]
    sends = []

    zs = [my_z]
    for i in range(nz - 1):
        value = jnp.int32(0)
        for z, others in enumerate(partners(nz)):
            value = jnp.where(my_z == z, others[i], value)
        zs.append(value)

    def slot(i, dx):
        return zs[i] * nx + dx

    def at(i, dx):
        return zs[i] * nx + lax.rem(my_x + dx, nx)

    def seen(dx):
        return my_z * nx + (nx - dx) % nx

    def remote(src, dst, sems, sent, got, ep_id, tp_id):
        return pltpu.make_async_remote_copy(
            src_ref=src,
            dst_ref=dst,
            send_sem=sems.at[(0,) + sent],
            recv_sem=sems.at[(1,) + got],
            device_id=(ep_id, tp_id),
            device_id_type=pl.DeviceIdType.MESH,
        )

    def to(src, dst, sems, index, ep_id, tp_id, got=None):
        copy = remote(src, dst, sems, index, index if got is None else got, ep_id, tp_id)
        copy.start()
        sends.append(copy)
        return copy

    def come(dst, sems, got):
        remote(dst, dst, sems, got, got, me, mate).wait_recv()

    def lane_block(t):
        return pl.ds(pl.multiple_of(t * columns, columns), columns)

    S = jax.named_scope

    barrier = pltpu.get_barrier_semaphore()
    for d in range(1, n_ep):
        pl.semaphore_signal(
            barrier,
            inc=1,
            device_id=(lax.rem(me + d, n_ep), tp),
            device_id_type=pl.DeviceIdType.MESH,
        )
    for d in range(1, n_tp):
        pl.semaphore_signal(
            barrier,
            inc=1,
            device_id=(me, lax.rem(tp + d, n_tp)),
            device_id_type=pl.DeviceIdType.MESH,
        )

    loads = []
    half_rows = pl.ds(pl.multiple_of(my_c * share, share), share)
    for i, (source, target) in enumerate(
        (
            (moe_hbm, moe_v),
            (ckv_hbm.at[half_rows], ckv_v),
            (q_hbm, qraw),
            (wg_hbm, wg),
            (wu_hbm, wu),
            (wd_hbm, wd),
            (wkv_hbm, wkv_ref),
            (wo_hbm, wo_ref),
        )
    ):
        copy = pltpu.make_async_copy(source, target, in_sem.at[i])
        loads.append(copy)
    loads[0].start()

    with S("routing"):
        top = routes_ref.shape[0]
        expert_of = lax.broadcasted_iota(jnp.int32, (n_ep, row_count), 0)
        named = jnp.zeros((n_ep, row_count), f32)
        mix = jnp.zeros((n_ep, row_count), f32)
        for k in range(top):
            hit = routes_ref[k : k + 1, :] == expert_of
            named = jnp.where(hit, 1.0, named)
            mix = jnp.where(hit, weight_ref[k : k + 1, :], mix)
        mix_ref[...] = mix
        first = lax.broadcasted_iota(jnp.int32, (row_count, row_count), 0)
        second = lax.broadcasted_iota(jnp.int32, (row_count, row_count), 1)
        before = jnp.where(first < second, 1.0, 0.0).astype(bf16)
        earlier = jnp.dot(named.astype(bf16), before, preferred_element_type=f32)
        key_ref[...] = jnp.where(named > 0.5, earlier, -1.0).astype(jnp.int32)
    place = lax.broadcasted_iota(jnp.int32, (cap, row_count), 0)

    def chosen(e):
        return key_ref[pl.ds(e, 1), :] == place

    def rows_for(e, cols):
        pick = jnp.where(chosen(e), 1.0, 0.0).astype(bf16)
        return jnp.dot(pick, normed[:, cols], preferred_element_type=f32).astype(bf16)

    with S("norm"):
        loads[0].wait()
        for copy in loads[1:]:
            copy.start()
        step_rows = 16

        def norm(i, carry):
            span = pl.ds(pl.multiple_of(i * step_rows, step_rows), step_rows)
            x = moe_v[span, :].astype(f32)
            level = lax.rsqrt(jnp.mean(x * x, axis=-1, keepdims=True) + EPSILON)
            normed[span, :] = (x * level * mgain_ref[...]).astype(bf16)
            return carry

        lax.fori_loop(0, row_count // step_rows, norm, 0, unroll=4)

    with S("gather_x"):
        for dx in range(1, nx):
            for o in range(n_y):
                out_x[dx, o] = rows_for(at(0, dx), lane_block(o * CORES + my_c))
    with S("barrier"):
        pl.semaphore_wait(barrier, n_ep + n_tp - 2)
    for dx in range(1, nx):
        for o in range(n_y):
            t = o * CORES + my_c
            to(
                out_x.at[dx, o],
                g_moe.at[t, seen(dx)],
                moe_x,
                (dx, o),
                at(0, dx),
                tp,
                ((nx - dx) % nx, o),
            )
    with S("gather_z"):
        for i in range(1, nz):
            for dx in range(nx):
                n = i * nx + dx
                out_z[n] = rows_for(at(i, dx), lane_block(tp))
                to(out_z.at[n], g_moe.at[tp, seen(dx)], moe_a, (n,), at(i, dx), tp, (seen(dx),))
    with S("gather_own"):
        for t in range(n_tp):
            g_moe[t, slot(0, 0)] = rows_for(me, slice(t * columns, (t + 1) * columns))

    with S("prep"):
        half = ROPE // 2
        pos = (me * row_count + lax.broadcasted_iota(jnp.int32, (half, row_count), 1)).astype(f32)
        band = lax.broadcasted_iota(jnp.int32, (half, row_count), 0)
        frequency = jnp.zeros((half, row_count), f32)
        for i in range(half):
            frequency = jnp.where(band == i, float(np.float32(frequency_of[i])), frequency)
        angle = pos * frequency
        cosine, sine = jnp.cos(angle), jnp.sin(angle)
        zero = lambda n: jnp.zeros((n, row_count), f32)
        rest = LANES - PLAIN_HEAD_DIM - ROPE
        cos_t = jnp.concatenate(
            [jnp.ones((PLAIN_HEAD_DIM, row_count), f32), cosine, cosine, zero(rest)], axis=0
        ).T
        down_t = jnp.concatenate([zero(PLAIN_HEAD_DIM), -sine, zero(half + rest)], axis=0).T
        up_t = jnp.concatenate([zero(PLAIN_HEAD_DIM + half), sine, zero(rest)], axis=0).T
        shared = rope_ref[...].astype(f32)
        first_half, second_half = shared[:half], shared[half:]
        rope_v[...] = jnp.concatenate(
            [
                zero(PLAIN_HEAD_DIM),
                first_half * cosine - second_half * sine,
                second_half * cosine + first_half * sine,
                zero(rest),
            ],
            axis=0,
        )
        own_lat = my_c * nx
        loads[1].wait()
        c = ckv_v[...].astype(f32)
        level = lax.rsqrt(jnp.mean(c * c, axis=-1, keepdims=True) + EPSILON)
        own_block = g_lat.at[own_lat, my_z]
        own_block[:, :latent] = (c * level * lgain_ref[...]).astype(bf16)
        own_block[:, latent:] = rope_v[:, half_rows].T.astype(bf16)
        loads[2].wait()
        width = PLAIN_HEAD_DIM + ROPE
        for h in range(heads):
            start = (h * width) // LANES * LANES
            shift = h * width - start
            size = LANES if shift + width <= LANES else 2 * LANES
            x = qraw[:, start : start + size].astype(f32)
            if shift:
                x = pltpu.roll(x, size - shift, 1)
            x = x[:, :LANES]
            q_ref[:, h * LANES : (h + 1) * LANES] = (
                x * cos_t + pltpu.roll(x, LANES - half, 1) * down_t + pltpu.roll(x, half, 1) * up_t
            ).astype(bf16)

    lat_over, lat_side = {}, {}

    def lat_hop(d):
        if d == 0:
            src = g_lat.at[own_lat, my_z]

            @pl.when(my_z + 1 < nz)
            def _():
                remote(src, src, lat_up, (my_z,), (my_z,), me + nx, tp).start()

            @pl.when(my_z > 0)
            def _():
                remote(src, src, lat_dn, (my_z,), (my_z,), me - nx, tp).start()

            lat_share(my_z)
        else:
            @pl.when(my_z >= d)
            def _():
                z = my_z - d
                src = g_lat.at[own_lat, z]
                come(src, lat_up, (z,))

                @pl.when(my_z + 1 < nz)
                def _():
                    remote(src, src, lat_up, (z,), (z,), me + nx, tp).start()

                lat_share(z)

            @pl.when(my_z + d < nz)
            def _():
                z = my_z + d
                src = g_lat.at[own_lat, z]
                come(src, lat_dn, (z,))

                @pl.when(my_z > 0)
                def _():
                    remote(src, src, lat_dn, (z,), (z,), me - nx, tp).start()

                lat_share(z)

    def lat_share(z):
        mine = g_lat.at[own_lat, z]
        remote(mine, mine, lat_c, (0, z), (0, z), me, mate).start()
        if nx > 1:
            side = g_lat.at[own_lat + 1, z]
            remote(mine, side, lat_x, (z,), (z,), my_z * nx + 1 - my_x, tp).start()

    def lat_cross(z):
        if nx > 1:
            side = g_lat.at[own_lat + 1, z]
            come(side, lat_x, (z,))
            remote(side, side, lat_c, (1, z), (1, z), me, mate).start()

    def lat_done(z):
        for i in range(nx):
            come(g_lat.at[(1 - my_c) * nx + i, z], lat_c, (i, z))

    def lat_drain():
        for z in range(nz):
            block = g_lat.at[own_lat, z]

            @pl.when(jnp.logical_and(my_z >= z, my_z + 1 < nz))
            def _():
                remote(block, block, lat_up, (z,), (z,), me, mate).wait_send()

            @pl.when(jnp.logical_and(my_z <= z, my_z > 0))
            def _():
                remote(block, block, lat_dn, (z,), (z,), me, mate).wait_send()

            remote(block, block, lat_c, (0, z), (0, z), me, mate).wait_send()
            if nx > 1:
                side = g_lat.at[own_lat + 1, z]
                remote(block, block, lat_x, (z,), (z,), me, mate).wait_send()
                remote(side, side, lat_c, (1, z), (1, z), me, mate).wait_send()

    relay_y, relay_c = {}, {}

    def x_arrive():
        for dx in range(1, nx):
            relay_c[0, dx] = []
            for o in range(n_y):
                block = g_moe.at[o * CORES + my_c, slot(0, dx)]
                come(block, moe_x, (dx, o))
                relay_c[0, dx].append(to(block, block, moe_xc, (dx, o), me, mate))

    def spread(i, dx):
        n = i * nx + dx
        block = g_moe.at[tp, slot(i, dx)]
        come(block, moe_a, (slot(i, dx),))
        for o in range(1, n_y):
            other = lax.rem(my_y + o, n_y) * CORES + my_c
            relay_y[n, o] = to(block, block, moe_y, (o, n), me, other)
        relay_c[i, dx] = [to(block, block, moe_c, (0, n), me, mate)]

    def forward(i, dx):
        n = i * nx + dx
        for o in range(1, n_y):
            relay_y[n, o].wait_recv()
            came = g_moe.at[lax.rem(my_y + n_y - o, n_y) * CORES + my_c, slot(i, dx)]
            relay_c[i, dx].append(to(came, came, moe_c, (o, n), me, mate))

    def finish(i):
        for dx in range(nx):
            for copy in relay_c.get((i, dx), ()):
                copy.wait_recv()

    def up(c, f):
        span = slice(f * tile, (f + 1) * tile)
        gate = jnp.zeros((rows, tile), f32)
        lift = jnp.zeros((rows, tile), f32)
        for t in range(n_tp):
            x = merge_rows(g_moe[t, pl.ds(zs[c] * nx, nx)])
            gate += jnp.dot(
                x, wg[t * columns : (t + 1) * columns, span], preferred_element_type=f32
            )
            lift += jnp.dot(
                x, wu[t * columns : (t + 1) * columns, span], preferred_element_type=f32
            )
        hidden[:, span] = (gate / (1.0 + jnp.exp(-gate)) * lift).astype(bf16)

    reduce_c, reduce_y = {}, {}

    def down(c):
        for o in list(range(1, n_y)) + [0]:
            y = lax.rem(my_y + o, n_y)
            for mine in range(2):
                t = y * CORES + (my_c if mine else 1 - my_c)
                part[t, c] = (
                    jnp.dot(hidden[...], wd[:, lane_block(t)], preferred_element_type=f32)
                    .astype(bf16)
                    .reshape(nx, cap, columns)
                )
                if not mine:
                    reduce_c[c, o] = to(part.at[t, c], r1.at[o, c], red_c, (o, c), me, mate)

    def level_two(c):
        for o in range(1, n_y):
            y = lax.rem(my_y + o, n_y)
            reduce_c[c, o].wait_recv()
            for dx in range(nx):
                n = c * nx + dx
                s2[o, c, dx] = (
                    part[y * CORES + my_c, c, dx].astype(f32) + r1[o, c, dx].astype(f32)
                ).astype(bf16)
                reduce_y[n, o] = to(
                    s2.at[o, c, dx], r2.at[o, c, dx], red_y, (o, n), me, y * CORES + my_c
                )

    def give_back(c):
        reduce_c[c, 0].wait_recv()
        for dx in range(nx):
            n = c * nx + dx
            total = part[tp, c, dx].astype(f32) + r1[0, c, dx].astype(f32)
            for o in range(1, n_y):
                reduce_y[n, o].wait_recv()
                total += r2[o, c, dx].astype(f32)
            tot[n] = total.astype(bf16)
            if n > 0:
                to(tot.at[n], back.at[seen(dx)], ret_a, (n,), at(c, dx), tp, (seen(dx),))

    def combine(i, dx):
        if i == 0 and dx == 0:
            came = tot[0]
        else:
            come(back.at[slot(i, dx)], ret_a, (slot(i, dx),))
            came = back[slot(i, dx)]
        e = at(i, dx)
        weight = jnp.where(chosen(e), mix_ref[pl.ds(e, 1), :], 0.0)
        high = weight.astype(bf16)
        low = (weight - high.astype(f32)).astype(bf16)
        add = lax.dot_general(
            jnp.concatenate([high, low], axis=0),
            jnp.concatenate([came, came], axis=0),
            (((0,), (0,)), ((), ())),
            preferred_element_type=f32,
        )
        if i == 0 and dx == 0:
            exp_out[...] = add
        else:
            exp_out[...] += add

    block = nz * share

    def expand(t, carry):
        kv[pl.ds(pl.multiple_of(t * block, block), block), :] = jnp.dot(
            merge_rows(g_lat[t])[:, :latent], wkv_ref[...], preferred_element_type=f32
        ).astype(bf16)
        return carry

    whole_lat = g_lat.reshape(g_lat.shape[0] * block, g_lat.shape[3])
    lane = lax.broadcasted_iota(jnp.int32, (1, LANES), 1)
    packed = 2 if heads % 2 == 0 else 1
    parts = heads // packed
    att_in, att_mate = [], []

    def attend(part_index):
        for h in range(part_index * packed, (part_index + 1) * packed):
            head = kv[:, h * LANES : (h + 1) * LANES]
            keys = jnp.where(lane < PLAIN_HEAD_DIM, head, whole_lat[:, latent : latent + LANES])
            scores = (
                lax.dot_general(
                    q_ref[:, h * LANES : (h + 1) * LANES],
                    keys,
                    (((1,), (1,)), ((), ())),
                    preferred_element_type=f32,
                )
                * scale
            )
            peak = jnp.max(scores, axis=-1, keepdims=True)
            e = jnp.exp(scores - peak)
            total = jnp.sum(e, axis=-1, keepdims=True)
            mixed = jnp.dot(e.astype(bf16), head, preferred_element_type=f32) / total
            if packed == 1:
                mixed = jnp.where(lane < PLAIN_HEAD_DIM, 0.0, mixed)
            elif h % 2 == 0:
                held = pltpu.roll(mixed, VALUE_HEAD_DIM, 1)
            else:
                mixed = jnp.where(lane < VALUE_HEAD_DIM, held, mixed)
        g_att[tp, part_index] = mixed.astype(bf16)

    def att_send(p):
        own = g_att.at[tp, p]
        for o in range(1, n_y):
            other = lax.rem(my_y + o, n_y) * CORES + my_c
            att_in.append((p, o, to(own, own, att_y, (o, p), me, other)))
        att_mate.append(to(own, own, att_c, (0, p), me, mate))

    def att_forward(part_index):
        for p, o, copy in att_in:
            if p == part_index:
                copy.wait_recv()
                came = g_att.at[lax.rem(my_y + n_y - o, n_y) * CORES + my_c, p]
                att_mate.append(to(came, came, att_c, (o, p), me, mate))

    def project():
        for copy in att_mate:
            copy.wait_recv()
        total = jnp.zeros(att_out.shape, f32)
        for t in range(n_tp):
            x = jnp.concatenate([g_att[t, p] for p in range(g_att.shape[1])], axis=1)
            width = x.shape[1]
            total += jnp.dot(x, wo_ref[t * width : (t + 1) * width, :], preferred_element_type=f32)
        att_out[...] = total

    def weights_in():
        for copy in loads[3:]:
            copy.wait()

    def scoped(name, f, *a):
        with S(name):
            f(*a)

    def each(name, f, i):
        for dx in range(nx):
            scoped("%s%d%d" % (name, i, dx), f, i, dx)

    def half_up(c, k):
        for f in range(tiles):
            if (2 * f) // tiles == k:
                scoped("up%d_%d" % (c, f), up, c, f)

    last = nz - 1
    scoped("x_arrive", x_arrive)
    if nz > 1:
        each("spread", spread, 1)
    scoped("weights", weights_in)
    lat_next = 0
    for c in range(nz):
        scoped("finish%d" % c, finish, c)
        half_up(c, 0)
        if c == 0 and nz > 1:
            scoped("forward10", forward, 1, 0)
        if 1 <= c and 2 < c + 1 < nz + 0:
            scoped("spread%d0" % (c + 1), spread, c + 1, 0)
        half_up(c, 1)
        if 1 <= c and 2 < c + 1 < nz + 0:
            for dx in range(1, nx):
                scoped("spread%d%d" % (c + 1, dx), spread, c + 1, dx)
        if c > 0:
            scoped("level_two%d" % (c - 1), level_two, c - 1)
        scoped("down%d" % c, down, c)
        if c == 0 and nz > 1:
            for dx in range(1, nx):
                scoped("forward1%d" % dx, forward, 1, dx)
        if 1 <= c and 2 < c + 1 < nz + 0:
            each("forward", forward, c + 1)
        if c == 0 and nz > 2:
            each("spread", spread, 2)
            each("forward", forward, 2)
        if c > 0:
            scoped("give_back%d" % (c - 1), give_back, c - 1)
            scoped("lat%d" % lat_next, lat_hop, lat_next)
            lat_next += 1
    scoped("level_two%d" % last, level_two, last)
    while lat_next < nz:
        scoped("lat%d" % lat_next, lat_hop, lat_next)
        lat_next += 1
    scoped("give_back%d" % last, give_back, last)
    each("combine", combine, 0)
    for z in range(nz):
        scoped("cross%d" % z, lat_cross, z)
    for z in range(nz):
        scoped("lat_done%d" % z, lat_done, z)
    with S("expand"):
        lax.fori_loop(0, g_lat.shape[0], expand, 0)
    for p in range(parts):
        scoped("attend%d" % p, attend, p)
        att_send(p)
    for i in range(1, nz - 1):
        each("combine", combine, i)
    for p in range(parts):
        scoped("att_forward%d" % p, att_forward, p)
    scoped("project", project)
    if nz > 1:
        each("combine", combine, last)
    for copy in sends:
        copy.wait_send()
    lat_drain()


def local(
    queries,
    compressed_key_value,
    rope_key,
    latent_norm_gain,
    latent_to_key_value,
    out_proj,
    moe_input,
    moe_gain,
    routes,
    route_weight,
    gate_weight,
    up_weight,
    down_weight,
):
    n_ep = lax.axis_size("ep")
    n_tp = lax.axis_size("tp")
    n_y = n_tp // CORES
    bf16 = jnp.bfloat16
    row_count = queries.shape[0]
    heads = latent_to_key_value.shape[1] // (PLAIN_HEAD_DIM + VALUE_HEAD_DIM)
    latent = compressed_key_value.shape[1]
    share = row_count // CORES
    nx, nz = ep_shape(n_ep)
    over = -queries.shape[1] % LANES
    if over:
        queries = jnp.pad(queries, ((0, 0), (0, over)))
    if heads % 2 == 0:
        wo = out_proj
        parts = heads // 2
    else:
        wo = out_proj.reshape(n_tp * heads, VALUE_HEAD_DIM, out_proj.shape[1])
        wo = jnp.concatenate([jnp.zeros_like(wo), wo], axis=1)
        wo = wo.reshape(n_tp * heads * LANES, out_proj.shape[1])
        parts = heads
    model_width = moe_input.shape[1]
    capacity = 3 * row_count // n_ep
    places = -(-capacity // 16) * 16
    columns = model_width // n_tp
    ff = gate_weight.shape[2]
    vmem = pl.BlockSpec(memory_space=pltpu.VMEM)
    hbm = pl.BlockSpec(memory_space=pltpu.HBM)
    dma = lambda *shape: pltpu.SemaphoreType.DMA((2,) + shape)
    attention, experts = pl.pallas_call(
        functools.partial(fused, n_ep, n_tp, heads, (PLAIN_HEAD_DIM + ROPE) ** (-0.5)),
        out_shape=(
            jax.ShapeDtypeStruct((row_count, out_proj.shape[1]), jnp.float32),
            jax.ShapeDtypeStruct((row_count, columns), jnp.float32),
        ),
        in_specs=[vmem] * 5 + [hbm] * 8,
        out_specs=(vmem, vmem),
        scratch_shapes=[
            pltpu.VMEM((row_count, model_width), bf16),
            pltpu.VMEM((share, latent), bf16),
            pltpu.VMEM(queries.shape, bf16),
            pltpu.VMEM(latent_to_key_value.shape, bf16),
            pltpu.VMEM(wo.shape, bf16),
            pltpu.VMEM((model_width, ff), bf16),
            pltpu.VMEM((model_width, ff), bf16),
            pltpu.VMEM((ff, model_width), bf16),
            pltpu.VMEM((row_count, model_width), bf16),
            pltpu.VMEM((n_ep, row_count), jnp.int32),
            pltpu.VMEM((n_ep, row_count), jnp.float32),
            pltpu.VMEM((n_ep, places, columns), bf16),
            pltpu.VMEM((nx, n_y, places, columns), bf16),
            pltpu.VMEM((LANES, row_count), jnp.float32),
            pltpu.VMEM((row_count, heads * LANES), bf16),
            pltpu.VMEM((CORES * nx, nz, share, latent + LANES), bf16),
            pltpu.VMEM((n_tp, n_ep, places, columns), bf16),
            pltpu.VMEM((n_tp, parts, row_count, LANES), bf16),
            pltpu.VMEM((n_ep * row_count, heads * LANES), bf16),
            pltpu.VMEM((nx * places, ff), bf16),
            pltpu.VMEM((n_tp, nz, nx, places, columns), bf16),
            pltpu.VMEM((n_y, nz, nx, places, columns), bf16),
            pltpu.VMEM((n_y, nz, nx, places, columns), bf16),
            pltpu.VMEM((n_y, nz, nx, places, columns), bf16),
            pltpu.VMEM((n_ep, places, columns), bf16),
            pltpu.VMEM((n_ep, places, columns), bf16),
            pltpu.SemaphoreType.DMA((8,)),
            dma(nz),
            dma(nz),
            dma(nz),
            dma(nx, nz),
            dma(n_ep),
            dma(nx, n_y),
            dma(nx, n_y),
            dma(n_y, n_ep),
            dma(n_y, n_ep),
            dma(n_y, parts),
            dma(n_y, parts),
            dma(n_y, nz),
            dma(n_y, n_ep),
            dma(n_ep),
        ],
        compiler_params=pltpu.CompilerParams(
            collective_id=0, has_side_effects=True, vmem_limit_bytes=50 * 1024 * 1024
        ),
        name="fused",
    )(
        routes.T,
        route_weight.T,
        moe_gain.reshape(1, model_width),
        latent_norm_gain.reshape(1, latent),
        rope_key.T,
        moe_input,
        compressed_key_value,
        queries,
        latent_to_key_value,
        wo,
        gate_weight.reshape(model_width, ff),
        up_weight.reshape(model_width, ff),
        down_weight.reshape(ff, model_width),
    )
    return attention.astype(bf16), experts.astype(bf16)


def solution(mesh):
    return jax.shard_map(
        local,
        mesh=mesh,
        in_specs=(
            P("ep", "tp"),
            P("ep", None),
            P("ep", None),
            P(),
            P(None, "tp"),
            P(None, "tp"),
            P("ep", None),
            P(),
            P("ep", None),
            P("ep", None),
            P("ep", None, "tp"),
            P("ep", None, "tp"),
            P("ep", "tp", None),
        ),
        out_specs=(P("ep", "tp"), P("ep", "tp")),
        check_vma=False,
    )
```

```python
import functools

import jax
import jax.numpy as jnp
import numpy as np
from jax import lax
from jax.experimental import pallas as pl
from jax.experimental.pallas import tpu as pltpu
from jax.sharding import PartitionSpec as P

PLAIN_HEAD_DIM = 64
ROPE = 32
VALUE_HEAD_DIM = 64
LANES = 128
CORES = 2


EPSILON = 1e-06
ROPE_BASE_VALUE = 10000.0


def ep_shape(n_ep):
    nx = 2 if n_ep % 2 == 0 else 1
    return nx, n_ep // nx


def partners(nz):
    side = lambda z: 2 * z < nz
    return [
        sorted(
            (o for o in range(nz) if o != z),
            key=lambda o: (abs(o - z), side(o) != side(z), o),
        )
        for z in range(nz)
    ]


def merge_rows(block):
    return block.reshape(block.shape[0] * block.shape[1], block.shape[2])


def fused(
    n_ep,
    n_tp,
    heads,
    scale,
    routes_hbm,
    weight_hbm,
    mgain_hbm,
    lgain_hbm,
    rope_hbm,
    moe_hbm,
    ckv_hbm,
    q_hbm,
    wkv_hbm,
    wo_hbm,
    wg_hbm,
    wu_hbm,
    wd_hbm,
    att_out,
    exp_out,
    routes_ref,
    weight_ref,
    mgain_ref,
    lgain_ref,
    rope_ref,
    moe_v,
    ckv_v,
    qraw,
    wkv_ref,
    wo_ref,
    wg,
    wu,
    wd,
    normed,
    key_ref,
    mix_ref,
    out_z,
    out_x,
    rope_v,
    q_ref,
    g_lat,
    g_moe,
    g_att,
    kv,
    hidden,
    part,
    r1,
    s2,
    r2,
    tot,
    back,
    in_sem,
    lat_up,
    lat_dn,
    lat_x,
    lat_c,
    moe_a,
    moe_x,
    moe_xc,
    moe_y,
    moe_c,
    att_y,
    att_c,
    red_c,
    red_y,
    ret_a,
):
    f32, bf16 = jnp.float32, jnp.bfloat16
    frequency_of = ROPE_BASE_VALUE ** (-np.arange(ROPE // 2, dtype=np.float32) * 2.0 / ROPE)
    me = lax.axis_index("ep")
    tp = lax.axis_index("tp")
    n_y = n_tp // CORES
    my_y = tp // CORES
    my_c = lax.rem(tp, CORES)
    mate = my_y * CORES + (1 - my_c)
    nx, nz = ep_shape(n_ep)
    my_z = me // nx
    my_x = lax.rem(me, nx)
    row_count, model_width = moe_v.shape
    columns = model_width // n_tp
    cap = g_moe.shape[2]
    chunks = nz
    rows = nx * cap
    ff = wg.shape[1]
    tile = min(256, ff)
    tiles = ff // tile
    share = ckv_v.shape[0]
    latent = ckv_v.shape[1]
    sends = []

    zs = [my_z]
    for i in range(nz - 1):
        value = jnp.int32(0)
        for z, others in enumerate(partners(nz)):
            value = jnp.where(my_z == z, others[i], value)
        zs.append(value)

    def slot(i, dx):
        return zs[i] * nx + dx

    def at(i, dx):
        return zs[i] * nx + lax.rem(my_x + dx, nx)

    def seen(dx):
        return my_z * nx + (nx - dx) % nx

    def remote(src, dst, sems, sent, got, ep_id, tp_id):
        return pltpu.make_async_remote_copy(
            src_ref=src,
            dst_ref=dst,
            send_sem=sems.at[(0,) + sent],
            recv_sem=sems.at[(1,) + got],
            device_id=(ep_id, tp_id),
            device_id_type=pl.DeviceIdType.MESH,
        )

    def to(src, dst, sems, index, ep_id, tp_id, got=None):
        copy = remote(src, dst, sems, index, index if got is None else got, ep_id, tp_id)
        copy.start()
        sends.append(copy)
        return copy

    def come(dst, sems, got):
        remote(dst, dst, sems, got, got, me, mate).wait_recv()

    def lane_block(t):
        return pl.ds(pl.multiple_of(t * columns, columns), columns)

    S = jax.named_scope

    def scoped(name, f, *a):
        with S(name):
            f(*a)

    barrier = pltpu.get_barrier_semaphore()
    for d in range(1, n_ep):
        pl.semaphore_signal(
            barrier,
            inc=1,
            device_id=(lax.rem(me + d, n_ep), tp),
            device_id_type=pl.DeviceIdType.MESH,
        )
    for d in range(1, n_tp):
        pl.semaphore_signal(
            barrier,
            inc=1,
            device_id=(me, lax.rem(tp + d, n_tp)),
            device_id_type=pl.DeviceIdType.MESH,
        )

    loads = []
    small = []
    for i, (source, target) in enumerate(
        (
            (routes_hbm, routes_ref),
            (weight_hbm, weight_ref),
            (mgain_hbm, mgain_ref),
            (lgain_hbm, lgain_ref),
            (rope_hbm, rope_ref),
        )
    ):
        copy = pltpu.make_async_copy(source, target, in_sem.at[8 + i])
        copy.start()
        small.append(copy)
    half_rows = pl.ds(pl.multiple_of(my_c * share, share), share)
    for i, (source, target) in enumerate(
        (
            (moe_hbm, moe_v),
            (ckv_hbm.at[half_rows], ckv_v),
            (q_hbm, qraw),
            (wg_hbm, wg),
            (wu_hbm, wu),
            (wd_hbm, wd),
            (wkv_hbm, wkv_ref),
            (wo_hbm, wo_ref),
        )
    ):
        copy = pltpu.make_async_copy(source, target, in_sem.at[i])
        loads.append(copy)
    loads[0].start()

    with S("routing"):
        for copy in small[:2]:
            copy.wait()
        top = routes_ref.shape[0]
        expert_of = lax.broadcasted_iota(jnp.int32, (n_ep, row_count), 0)
        named = jnp.zeros((n_ep, row_count), f32)
        mix = jnp.zeros((n_ep, row_count), f32)
        for k in range(top):
            hit = routes_ref[k : k + 1, :] == expert_of
            named = jnp.where(hit, 1.0, named)
            mix = jnp.where(hit, weight_ref[k : k + 1, :], mix)
        mix_ref[...] = mix
        first = lax.broadcasted_iota(jnp.int32, (row_count, row_count), 0)
        second = lax.broadcasted_iota(jnp.int32, (row_count, row_count), 1)
        before = jnp.where(first < second, 1.0, 0.0).astype(bf16)
        earlier = jnp.dot(named.astype(bf16), before, preferred_element_type=f32)
        key_ref[...] = jnp.where(named > 0.5, earlier, -1.0).astype(jnp.int32)
    place = lax.broadcasted_iota(jnp.int32, (cap, row_count), 0)

    def chosen(e):
        return key_ref[pl.ds(e, 1), :] == place

    def rows_for(e, cols):
        pick = jnp.where(chosen(e), 1.0, 0.0).astype(bf16)
        return jnp.dot(pick, normed[:, cols], preferred_element_type=f32).astype(bf16)

    with S("norm"):
        loads[0].wait()
        for copy in small[2:]:
            copy.wait()
        for copy in loads[1:]:
            copy.start()
        step_rows = 16

        def norm(i, carry):
            span = pl.ds(pl.multiple_of(i * step_rows, step_rows), step_rows)
            x = moe_v[span, :].astype(f32)
            level = lax.rsqrt(jnp.mean(x * x, axis=-1, keepdims=True) + EPSILON)
            normed[span, :] = (x * level * mgain_ref[...]).astype(bf16)
            return carry

        lax.fori_loop(0, row_count // step_rows, norm, 0, unroll=4)


    def direct(i, dx):
        return i == 0 or (i == 1 and dx == 0)

    sent = {}

    def gather(i, dx):
        n = i * nx + dx
        if direct(i, dx):
            for o in range(n_y):
                out_x[n, o] = rows_for(at(i, dx), lane_block(o * CORES + my_c))
        else:
            out_z[n] = rows_for(at(i, dx), lane_block(tp))

    def send(i, dx):
        n = i * nx + dx
        if direct(i, dx):
            sent[n] = [
                to(
                    out_x.at[n, o],
                    g_moe.at[o * CORES + my_c, seen(dx)],
                    moe_x,
                    (n, o),
                    at(i, dx),
                    tp,
                    (seen(dx), o),
                )
                for o in range(n_y)
            ]
        else:
            sent[n] = [
                to(out_z.at[n], g_moe.at[tp, seen(dx)], moe_a, (n,), at(i, dx), tp, (seen(dx),))
            ]

    def gone(i, dx):
        for copy in sent[i * nx + dx]:
            copy.wait_send()
            sends[:] = [other for other in sends if other is not copy]

    side = range(1, nx)
    with S("gather_a"):
        for dx in side:
            gather(0, dx)
        if nz > 1:
            gather(1, 0)
        if nz > 2:
            gather(2, 0)
    with S("barrier"):
        pl.semaphore_wait(barrier, n_ep + n_tp - 2)
    for dx in side:
        send(0, dx)
    for i in range(1, min(3, nz)):
        send(i, 0)
    with S("gather_b"):
        for i in range(1, nz):
            for dx in range(nx):
                if dx or i > 2:
                    gather(i, dx)
    with S("gather_own"):
        for t in range(n_tp):
            g_moe[t, slot(0, 0)] = rows_for(me, slice(t * columns, (t + 1) * columns))

    with S("prep"):
        half = ROPE // 2
        pos = (me * row_count + lax.broadcasted_iota(jnp.int32, (half, row_count), 1)).astype(f32)
        band = lax.broadcasted_iota(jnp.int32, (half, row_count), 0)
        frequency = jnp.zeros((half, row_count), f32)
        for i in range(half):
            frequency = jnp.where(band == i, float(np.float32(frequency_of[i])), frequency)
        angle = pos * frequency
        cosine, sine = jnp.cos(angle), jnp.sin(angle)
        zero = lambda n: jnp.zeros((n, row_count), f32)
        rest = LANES - PLAIN_HEAD_DIM - ROPE
        cos_t = jnp.concatenate(
            [jnp.ones((PLAIN_HEAD_DIM, row_count), f32), cosine, cosine, zero(rest)], axis=0
        ).T
        down_t = jnp.concatenate([zero(PLAIN_HEAD_DIM), -sine, zero(half + rest)], axis=0).T
        up_t = jnp.concatenate([zero(PLAIN_HEAD_DIM + half), sine, zero(rest)], axis=0).T
        shared = rope_ref[...].astype(f32)
        first_half, second_half = shared[:half], shared[half:]
        rope_v[...] = jnp.concatenate(
            [
                zero(PLAIN_HEAD_DIM),
                first_half * cosine - second_half * sine,
                second_half * cosine + first_half * sine,
                zero(rest),
            ],
            axis=0,
        )
        own_lat = my_c * nx
        loads[1].wait()
        c = ckv_v[...].astype(f32)
        level = lax.rsqrt(jnp.mean(c * c, axis=-1, keepdims=True) + EPSILON)
        own_block = g_lat.at[own_lat, my_z]
        own_block[:, :latent] = (c * level * lgain_ref[...]).astype(bf16)
        own_block[:, latent:] = rope_v[:, half_rows].T.astype(bf16)
        loads[2].wait()
        width = PLAIN_HEAD_DIM + ROPE
        for h in range(heads):
            start = (h * width) // LANES * LANES
            shift = h * width - start
            size = LANES if shift + width <= LANES else 2 * LANES
            x = qraw[:, start : start + size].astype(f32)
            if shift:
                x = pltpu.roll(x, size - shift, 1)
            x = x[:, :LANES]
            q_ref[:, h * LANES : (h + 1) * LANES] = (
                x * cos_t + pltpu.roll(x, LANES - half, 1) * down_t + pltpu.roll(x, half, 1) * up_t
            ).astype(bf16)

    lat_over, lat_side = {}, {}

    def lat_hop(d):
        if d == 0:
            src = g_lat.at[own_lat, my_z]

            @pl.when(my_z + 1 < nz)
            def _():
                remote(src, src, lat_up, (my_z,), (my_z,), me + nx, tp).start()

            @pl.when(my_z > 0)
            def _():
                remote(src, src, lat_dn, (my_z,), (my_z,), me - nx, tp).start()

            lat_share(my_z)
        else:
            @pl.when(my_z >= d)
            def _():
                z = my_z - d
                src = g_lat.at[own_lat, z]
                come(src, lat_up, (z,))

                @pl.when(my_z + 1 < nz)
                def _():
                    remote(src, src, lat_up, (z,), (z,), me + nx, tp).start()

                lat_share(z)

            @pl.when(my_z + d < nz)
            def _():
                z = my_z + d
                src = g_lat.at[own_lat, z]
                come(src, lat_dn, (z,))

                @pl.when(my_z > 0)
                def _():
                    remote(src, src, lat_dn, (z,), (z,), me - nx, tp).start()

                lat_share(z)

    def lat_share(z):
        mine = g_lat.at[own_lat, z]
        remote(mine, mine, lat_c, (0, z), (0, z), me, mate).start()
        if nx > 1:
            side = g_lat.at[own_lat + 1, z]
            remote(mine, side, lat_x, (z,), (z,), my_z * nx + 1 - my_x, tp).start()

    def lat_cross(z):
        if nx > 1:
            side = g_lat.at[own_lat + 1, z]
            come(side, lat_x, (z,))
            remote(side, side, lat_c, (1, z), (1, z), me, mate).start()

    def lat_done(z):
        for i in range(nx):
            come(g_lat.at[(1 - my_c) * nx + i, z], lat_c, (i, z))

    def lat_drain():
        for z in range(nz):
            block = g_lat.at[own_lat, z]

            @pl.when(jnp.logical_and(my_z >= z, my_z + 1 < nz))
            def _():
                remote(block, block, lat_up, (z,), (z,), me, mate).wait_send()

            @pl.when(jnp.logical_and(my_z <= z, my_z > 0))
            def _():
                remote(block, block, lat_dn, (z,), (z,), me, mate).wait_send()

            remote(block, block, lat_c, (0, z), (0, z), me, mate).wait_send()
            if nx > 1:
                side = g_lat.at[own_lat + 1, z]
                remote(block, block, lat_x, (z,), (z,), me, mate).wait_send()
                remote(side, side, lat_c, (1, z), (1, z), me, mate).wait_send()

    relay_y, relay_c = {}, {}

    def arrive(i, dx):
        relay_c[i, dx] = []
        for o in range(n_y):
            block = g_moe.at[o * CORES + my_c, slot(i, dx)]
            come(block, moe_x, (slot(i, dx), o))
            relay_c[i, dx].append(to(block, block, moe_xc, (i * nx + dx, o), me, mate))

    def spread(i, dx):
        n = i * nx + dx
        block = g_moe.at[tp, slot(i, dx)]
        come(block, moe_a, (slot(i, dx),))
        for o in range(1, n_y):
            other = lax.rem(my_y + o, n_y) * CORES + my_c
            relay_y[n, o] = to(block, block, moe_y, (o, n), me, other)
        relay_c[i, dx] = [to(block, block, moe_c, (0, n), me, mate)]

    def forward(i, dx):
        n = i * nx + dx
        for o in range(1, n_y):
            relay_y[n, o].wait_recv()
            came = g_moe.at[lax.rem(my_y + n_y - o, n_y) * CORES + my_c, slot(i, dx)]
            relay_c[i, dx].append(to(came, came, moe_c, (o, n), me, mate))

    def finish(i):
        for dx in range(nx):
            for copy in relay_c.get((i, dx), ()):
                copy.wait_recv()

    def up(c, f):
        span = slice(f * tile, (f + 1) * tile)
        gate = jnp.zeros((rows, tile), f32)
        lift = jnp.zeros((rows, tile), f32)
        for t in range(n_tp):
            x = merge_rows(g_moe[t, pl.ds(zs[c] * nx, nx)])
            gate += jnp.dot(
                x, wg[t * columns : (t + 1) * columns, span], preferred_element_type=f32
            )
            lift += jnp.dot(
                x, wu[t * columns : (t + 1) * columns, span], preferred_element_type=f32
            )
        hidden[:, span] = (gate / (1.0 + jnp.exp(-gate)) * lift).astype(bf16)

    reduce_c, reduce_y = {}, {}

    def down(c):
        for o in list(range(1, n_y)) + [0]:
            y = lax.rem(my_y + o, n_y)
            for mine in range(2):
                t = y * CORES + (my_c if mine else 1 - my_c)
                part[t, c] = (
                    jnp.dot(hidden[...], wd[:, lane_block(t)], preferred_element_type=f32)
                    .astype(bf16)
                    .reshape(nx, cap, columns)
                )
                if not mine:
                    reduce_c[c, o] = to(part.at[t, c], r1.at[o, c], red_c, (o, c), me, mate)

    def level_two(c):
        for o in range(1, n_y):
            y = lax.rem(my_y + o, n_y)
            reduce_c[c, o].wait_recv()
            for dx in range(nx):
                n = c * nx + dx
                s2[o, c, dx] = (
                    part[y * CORES + my_c, c, dx].astype(f32) + r1[o, c, dx].astype(f32)
                ).astype(bf16)
                reduce_y[n, o] = to(
                    s2.at[o, c, dx], r2.at[o, c, dx], red_y, (o, n), me, y * CORES + my_c
                )

    def give_back(c):
        reduce_c[c, 0].wait_recv()
        for dx in range(nx):
            n = c * nx + dx
            total = part[tp, c, dx].astype(f32) + r1[0, c, dx].astype(f32)
            for o in range(1, n_y):
                reduce_y[n, o].wait_recv()
                total += r2[o, c, dx].astype(f32)
            tot[n] = total.astype(bf16)
            if n > 0:
                to(tot.at[n], back.at[seen(dx)], ret_a, (n,), at(c, dx), tp, (seen(dx),))

    def combine(i, dx):
        if i == 0 and dx == 0:
            came = tot[0]
        else:
            come(back.at[slot(i, dx)], ret_a, (slot(i, dx),))
            came = back[slot(i, dx)]
        e = at(i, dx)
        weight = jnp.where(chosen(e), mix_ref[pl.ds(e, 1), :], 0.0)
        high = weight.astype(bf16)
        low = (weight - high.astype(f32)).astype(bf16)
        add = lax.dot_general(
            jnp.concatenate([high, low], axis=0),
            jnp.concatenate([came, came], axis=0),
            (((0,), (0,)), ((), ())),
            preferred_element_type=f32,
        )
        if i == 0 and dx == 0:
            exp_out[...] = add
        else:
            exp_out[...] += add

    block = nz * share

    def expand(t, carry):
        kv[pl.ds(pl.multiple_of(t * block, block), block), :] = jnp.dot(
            merge_rows(g_lat[t])[:, :latent], wkv_ref[...], preferred_element_type=f32
        ).astype(bf16)
        return carry

    whole_lat = g_lat.reshape(g_lat.shape[0] * block, g_lat.shape[3])
    lane = lax.broadcasted_iota(jnp.int32, (1, LANES), 1)
    packed = 2 if heads % 2 == 0 else 1
    parts = heads // packed
    att_in, att_mate = [], []

    def attend(part_index):
        for h in range(part_index * packed, (part_index + 1) * packed):
            head = kv[:, h * LANES : (h + 1) * LANES]
            keys = jnp.where(lane < PLAIN_HEAD_DIM, head, whole_lat[:, latent : latent + LANES])
            scores = (
                lax.dot_general(
                    q_ref[:, h * LANES : (h + 1) * LANES],
                    keys,
                    (((1,), (1,)), ((), ())),
                    preferred_element_type=f32,
                )
                * scale
            )
            peak = jnp.max(scores, axis=-1, keepdims=True)
            e = jnp.exp(scores - peak)
            total = jnp.sum(e, axis=-1, keepdims=True)
            mixed = jnp.dot(e.astype(bf16), head, preferred_element_type=f32) / total
            if packed == 1:
                mixed = jnp.where(lane < PLAIN_HEAD_DIM, 0.0, mixed)
            elif h % 2 == 0:
                held = pltpu.roll(mixed, VALUE_HEAD_DIM, 1)
            else:
                mixed = jnp.where(lane < VALUE_HEAD_DIM, held, mixed)
        g_att[tp, part_index] = mixed.astype(bf16)

    def att_send(p):
        own = g_att.at[tp, p]
        for o in range(1, n_y):
            other = lax.rem(my_y + o, n_y) * CORES + my_c
            att_in.append((p, o, to(own, own, att_y, (o, p), me, other)))
        att_mate.append(to(own, own, att_c, (0, p), me, mate))

    def att_forward(part_index):
        for p, o, copy in att_in:
            if p == part_index:
                copy.wait_recv()
                came = g_att.at[lax.rem(my_y + n_y - o, n_y) * CORES + my_c, p]
                att_mate.append(to(came, came, att_c, (o, p), me, mate))

    def project():
        for copy in att_mate:
            copy.wait_recv()
        total = jnp.zeros(att_out.shape, f32)
        for t in range(n_tp):
            x = jnp.concatenate([g_att[t, p] for p in range(g_att.shape[1])], axis=1)
            width = x.shape[1]
            total += jnp.dot(x, wo_ref[t * width : (t + 1) * width, :], preferred_element_type=f32)
        att_out[...] = total

    def weights_in():
        for copy in loads[3:]:
            copy.wait()

    def each(name, f, i, some=range(nx)):
        for dx in some:
            scoped("%s%d%d" % (name, i, dx), f, i, dx)

    def half_up(c, k):
        for f in range(tiles):
            if (2 * f) // tiles == k:
                scoped("up%d_%d" % (c, f), up, c, f)

    last = nz - 1
    each("gone", gone, 0, side)
    for i in range(1, min(3, nz)):
        each("send", send, i, side)
    for i in range(3, nz):
        send(i, 0)
    each("arrive", arrive, 0, side)
    scoped("weights", weights_in)
    if nz > 1:
        each("arrive", arrive, 1, range(1))
    scoped("finish0", finish, 0)
    half_up(0, 0)
    for i in range(3, nz):
        each("send", send, i, side)
    half_up(0, 1)
    scoped("down0", down, 0)
    if nz > 1:
        each("spread", spread, 1, side)
        scoped("level_two0", level_two, 0)
        each("forward", forward, 1, side)
        scoped("finish1", finish, 1)
        half_up(1, 0)
    scoped("lat0", lat_hop, 0)
    if nz > 2:
        each("spread", spread, 2)
    if nz > 1:
        half_up(1, 1)
    for i in range(3, nz):
        each("spread", spread, i)
    if nz > 1:
        scoped("down1", down, 1)
        scoped("lat1", lat_hop, 1)
        if nz > 2:
            each("forward", forward, 2)
        scoped("level_two1", level_two, 1)
        scoped("give_back0", give_back, 0)
    for c in range(2, nz):
        scoped("finish%d" % c, finish, c)
        half_up(c, 0)
        if c + 1 < nz:
            each("forward", forward, c + 1, range(1))
        scoped("lat%d" % c, lat_hop, c)
        half_up(c, 1)
        if c + 1 < nz:
            each("forward", forward, c + 1, side)
        scoped("down%d" % c, down, c)
        scoped("level_two%d" % c, level_two, c)
        scoped("give_back%d" % (c - 1), give_back, c - 1)
    for z in range(nz):
        scoped("cross%d" % z, lat_cross, z)
    each("combine", combine, 0)
    for z in range(nz):
        scoped("lat_done%d" % z, lat_done, z)
    with S("expand"):
        lax.fori_loop(0, g_lat.shape[0], expand, 0)
    scoped("give_back%d" % last, give_back, last)
    for p in range(parts):
        scoped("attend%d" % p, attend, p)
        att_send(p)
    for p in range(parts):
        scoped("att_forward%d" % p, att_forward, p)
    scoped("project", project)
    for i in range(1, nz):
        each("combine", combine, i)
    for copy in sends:
        copy.wait_send()
    lat_drain()


def local(
    queries,
    compressed_key_value,
    rope_key,
    latent_norm_gain,
    latent_to_key_value,
    out_proj,
    moe_input,
    moe_gain,
    routes,
    route_weight,
    gate_weight,
    up_weight,
    down_weight,
):
    n_ep = lax.axis_size("ep")
    n_tp = lax.axis_size("tp")
    n_y = n_tp // CORES
    bf16 = jnp.bfloat16
    row_count = queries.shape[0]
    heads = latent_to_key_value.shape[1] // (PLAIN_HEAD_DIM + VALUE_HEAD_DIM)
    latent = compressed_key_value.shape[1]
    share = row_count // CORES
    nx, nz = ep_shape(n_ep)
    over = -queries.shape[1] % LANES
    if over:
        queries = jnp.pad(queries, ((0, 0), (0, over)))
    if heads % 2 == 0:
        wo = out_proj
        parts = heads // 2
    else:
        wo = out_proj.reshape(n_tp * heads, VALUE_HEAD_DIM, out_proj.shape[1])
        wo = jnp.concatenate([jnp.zeros_like(wo), wo], axis=1)
        wo = wo.reshape(n_tp * heads * LANES, out_proj.shape[1])
        parts = heads
    model_width = moe_input.shape[1]
    top = routes.shape[1]
    capacity = 3 * row_count // n_ep
    places = -(-capacity // 16) * 16
    columns = model_width // n_tp
    ff = gate_weight.shape[2]
    vmem = pl.BlockSpec(memory_space=pltpu.VMEM)
    hbm = pl.BlockSpec(memory_space=pltpu.HBM)
    dma = lambda *shape: pltpu.SemaphoreType.DMA((2,) + shape)
    attention, experts = pl.pallas_call(
        functools.partial(fused, n_ep, n_tp, heads, (PLAIN_HEAD_DIM + ROPE) ** (-0.5)),
        out_shape=(
            pltpu.VMEM((row_count, out_proj.shape[1]), jnp.float32),
            pltpu.VMEM((row_count, columns), jnp.float32),
        ),
        in_specs=[hbm] * 13,
        out_specs=(vmem, vmem),
        scratch_shapes=[
            pltpu.VMEM((top, row_count), jnp.int32),
            pltpu.VMEM((top, row_count), jnp.float32),
            pltpu.VMEM((1, model_width), jnp.float32),
            pltpu.VMEM((1, latent), jnp.float32),
            pltpu.VMEM((ROPE, row_count), bf16),
            pltpu.VMEM((row_count, model_width), bf16),
            pltpu.VMEM((share, latent), bf16),
            pltpu.VMEM(queries.shape, bf16),
            pltpu.VMEM(latent_to_key_value.shape, bf16),
            pltpu.VMEM(wo.shape, bf16),
            pltpu.VMEM((model_width, ff), bf16),
            pltpu.VMEM((model_width, ff), bf16),
            pltpu.VMEM((ff, model_width), bf16),
            pltpu.VMEM((row_count, model_width), bf16),
            pltpu.VMEM((n_ep, row_count), jnp.int32),
            pltpu.VMEM((n_ep, row_count), jnp.float32),
            pltpu.VMEM((n_ep, places, columns), bf16),
            pltpu.VMEM((min(2, nz) * nx, n_y, places, columns), bf16),
            pltpu.VMEM((LANES, row_count), jnp.float32),
            pltpu.VMEM((row_count, heads * LANES), bf16),
            pltpu.VMEM((CORES * nx, nz, share, latent + LANES), bf16),
            pltpu.VMEM((n_tp, n_ep, places, columns), bf16),
            pltpu.VMEM((n_tp, parts, row_count, LANES), bf16),
            pltpu.VMEM((n_ep * row_count, heads * LANES), bf16),
            pltpu.VMEM((nx * places, ff), bf16),
            pltpu.VMEM((n_tp, nz, nx, places, columns), bf16),
            pltpu.VMEM((n_y, nz, nx, places, columns), bf16),
            pltpu.VMEM((n_y, nz, nx, places, columns), bf16),
            pltpu.VMEM((n_y, nz, nx, places, columns), bf16),
            pltpu.VMEM((n_ep, places, columns), bf16),
            pltpu.VMEM((n_ep, places, columns), bf16),
            pltpu.SemaphoreType.DMA((13,)),
            dma(nz),
            dma(nz),
            dma(nz),
            dma(nx, nz),
            dma(n_ep),
            dma(n_ep, n_y),
            dma(n_ep, n_y),
            dma(n_y, n_ep),
            dma(n_y, n_ep),
            dma(n_y, parts),
            dma(n_y, parts),
            dma(n_y, nz),
            dma(n_y, n_ep),
            dma(n_ep),
        ],
        compiler_params=pltpu.CompilerParams(
            collective_id=0, has_side_effects=True, vmem_limit_bytes=60 * 1024 * 1024
        ),
        name="fused",
    )(
        routes.T,
        route_weight.T,
        moe_gain.reshape(1, model_width),
        latent_norm_gain.reshape(1, latent),
        rope_key.T,
        moe_input,
        compressed_key_value,
        queries,
        latent_to_key_value,
        wo,
        gate_weight.reshape(model_width, ff),
        up_weight.reshape(model_width, ff),
        down_weight.reshape(ff, model_width),
    )
    return attention.astype(bf16), experts.astype(bf16)


def solution(mesh):
    return jax.shard_map(
        local,
        mesh=mesh,
        in_specs=(
            P("ep", "tp"),
            P("ep", None),
            P("ep", None),
            P(),
            P(None, "tp"),
            P(None, "tp"),
            P("ep", None),
            P(),
            P("ep", None),
            P("ep", None),
            P("ep", None, "tp"),
            P("ep", None, "tp"),
            P("ep", "tp", None),
        ),
        out_specs=(P("ep", "tp"), P("ep", "tp")),
        check_vma=False,
    )
```

```python
import functools

import jax
import jax.numpy as jnp
import numpy as np
from jax import lax
from jax.experimental import pallas as pl
from jax.experimental.pallas import tpu as pltpu
from jax.sharding import PartitionSpec as P

PLAIN_HEAD_DIM = 64
ROPE = 32
VALUE_HEAD_DIM = 64
LANES = 128
CORES = 2


EPSILON = 1e-06
ROPE_BASE_VALUE = 10000.0


def ep_shape(n_ep):
    nx = 2 if n_ep % 2 == 0 else 1
    return nx, n_ep // nx


def partners(nz):
    side = lambda z: 2 * z < nz
    return [
        sorted(
            (o for o in range(nz) if o != z),
            key=lambda o: (abs(o - z), side(o) != side(z), o),
        )
        for z in range(nz)
    ]


def merge_rows(block):
    return block.reshape(block.shape[0] * block.shape[1], block.shape[2])


def fused(
    n_ep,
    n_tp,
    heads,
    scale,
    routes_hbm,
    weight_hbm,
    mgain_hbm,
    lgain_hbm,
    rope_hbm,
    moe_hbm,
    ckv_hbm,
    q_hbm,
    wkv_hbm,
    wo_hbm,
    wg_hbm,
    wu_hbm,
    wd_hbm,
    att_dst,
    exp_dst,
    routes_ref,
    weight_ref,
    mgain_ref,
    lgain_ref,
    rope_ref,
    moe_v,
    ckv_v,
    qraw,
    wkv_ref,
    wo_ref,
    wg,
    wu,
    wd,
    normed,
    key_ref,
    mix_ref,
    out_z,
    out_x,
    rope_v,
    q_ref,
    g_lat,
    g_moe,
    g_att,
    kv,
    hidden,
    part,
    r1,
    s2,
    r2,
    tot,
    back,
    acc,
    att_v,
    exp_v,
    in_sem,
    lat_up,
    lat_dn,
    lat_x,
    lat_c,
    moe_a,
    moe_x,
    moe_xc,
    moe_y,
    moe_c,
    att_y,
    att_c,
    red_c,
    red_y,
    ret_a,
):
    f32, bf16 = jnp.float32, jnp.bfloat16
    frequency_of = ROPE_BASE_VALUE ** (-np.arange(ROPE // 2, dtype=np.float32) * 2.0 / ROPE)
    me = lax.axis_index("ep")
    tp = lax.axis_index("tp")
    n_y = n_tp // CORES
    my_y = tp // CORES
    my_c = lax.rem(tp, CORES)
    mate = my_y * CORES + (1 - my_c)
    nx, nz = ep_shape(n_ep)
    my_z = me // nx
    my_x = lax.rem(me, nx)
    row_count, model_width = moe_v.shape
    columns = model_width // n_tp
    cap = g_moe.shape[2]
    chunks = nz
    rows = nx * cap
    ff = wg.shape[1]
    tile = min(256, ff)
    tiles = ff // tile
    share = ckv_v.shape[0]
    latent = ckv_v.shape[1]
    sends = []

    zs = [my_z]
    for i in range(nz - 1):
        value = jnp.int32(0)
        for z, others in enumerate(partners(nz)):
            value = jnp.where(my_z == z, others[i], value)
        zs.append(value)

    def slot(i, dx):
        return zs[i] * nx + dx

    def at(i, dx):
        return zs[i] * nx + lax.rem(my_x + dx, nx)

    def seen(dx):
        return my_z * nx + (nx - dx) % nx

    def remote(src, dst, sems, sent, got, ep_id, tp_id):
        return pltpu.make_async_remote_copy(
            src_ref=src,
            dst_ref=dst,
            send_sem=sems.at[(0,) + sent],
            recv_sem=sems.at[(1,) + got],
            device_id=(ep_id, tp_id),
            device_id_type=pl.DeviceIdType.MESH,
        )

    def to(src, dst, sems, index, ep_id, tp_id, got=None):
        copy = remote(src, dst, sems, index, index if got is None else got, ep_id, tp_id)
        copy.start()
        sends.append(copy)
        return copy

    def come(dst, sems, got):
        remote(dst, dst, sems, got, got, me, mate).wait_recv()

    def lane_block(t):
        return pl.ds(pl.multiple_of(t * columns, columns), columns)

    S = jax.named_scope

    def scoped(name, f, *a):
        with S(name):
            f(*a)

    barrier = pltpu.get_barrier_semaphore()
    for d in range(1, n_ep):
        pl.semaphore_signal(
            barrier,
            inc=1,
            device_id=(lax.rem(me + d, n_ep), tp),
            device_id_type=pl.DeviceIdType.MESH,
        )
    for d in range(1, n_tp):
        pl.semaphore_signal(
            barrier,
            inc=1,
            device_id=(me, lax.rem(tp + d, n_tp)),
            device_id_type=pl.DeviceIdType.MESH,
        )

    loads = []
    small = []
    for i, (source, target) in enumerate(
        (
            (routes_hbm, routes_ref),
            (weight_hbm, weight_ref),
            (mgain_hbm, mgain_ref),
            (lgain_hbm, lgain_ref),
            (rope_hbm, rope_ref),
        )
    ):
        copy = pltpu.make_async_copy(source, target, in_sem.at[8 + i])
        copy.start()
        small.append(copy)
    half_rows = pl.ds(pl.multiple_of(my_c * share, share), share)
    for i, (source, target) in enumerate(
        (
            (moe_hbm, moe_v),
            (ckv_hbm.at[half_rows], ckv_v),
            (q_hbm, qraw),
            (wg_hbm, wg),
            (wu_hbm, wu),
            (wd_hbm, wd),
            (wkv_hbm, wkv_ref),
            (wo_hbm, wo_ref),
        )
    ):
        copy = pltpu.make_async_copy(source, target, in_sem.at[i])
        loads.append(copy)
    loads[0].start()

    with S("routing"):
        for copy in small[:2]:
            copy.wait()
        top = routes_ref.shape[0]
        expert_of = lax.broadcasted_iota(jnp.int32, (n_ep, row_count), 0)
        named = jnp.zeros((n_ep, row_count), f32)
        mix = jnp.zeros((n_ep, row_count), f32)
        for k in range(top):
            hit = routes_ref[k : k + 1, :] == expert_of
            named = jnp.where(hit, 1.0, named)
            mix = jnp.where(hit, weight_ref[k : k + 1, :], mix)
        mix_ref[...] = mix
        first = lax.broadcasted_iota(jnp.int32, (row_count, row_count), 0)
        second = lax.broadcasted_iota(jnp.int32, (row_count, row_count), 1)
        before = jnp.where(first < second, 1.0, 0.0).astype(bf16)
        earlier = jnp.dot(named.astype(bf16), before, preferred_element_type=f32)
        key_ref[...] = jnp.where(named > 0.5, earlier, -1.0).astype(jnp.int32)
    place = lax.broadcasted_iota(jnp.int32, (cap, row_count), 0)

    def chosen(e):
        return key_ref[pl.ds(e, 1), :] == place

    def rows_for(e, cols):
        pick = jnp.where(chosen(e), 1.0, 0.0).astype(bf16)
        return jnp.dot(pick, normed[:, cols], preferred_element_type=f32).astype(bf16)

    with S("norm"):
        loads[0].wait()
        for copy in small[2:]:
            copy.wait()
        for copy in loads[1:]:
            copy.start()
        step_rows = 16

        def norm(i, carry):
            span = pl.ds(pl.multiple_of(i * step_rows, step_rows), step_rows)
            x = moe_v[span, :].astype(f32)
            level = lax.rsqrt(jnp.mean(x * x, axis=-1, keepdims=True) + EPSILON)
            normed[span, :] = (x * level * mgain_ref[...]).astype(bf16)
            return carry

        lax.fori_loop(0, row_count // step_rows, norm, 0, unroll=4)


    def direct(i, dx):
        return i == 0

    sent = {}

    def gather(i, dx):
        n = i * nx + dx
        if direct(i, dx):
            for o in range(n_y):
                out_x[n, o] = rows_for(at(i, dx), lane_block(o * CORES + my_c))
        else:
            out_z[n] = rows_for(at(i, dx), lane_block(tp))

    def send(i, dx):
        n = i * nx + dx
        if direct(i, dx):
            sent[n] = [
                to(
                    out_x.at[n, o],
                    g_moe.at[o * CORES + my_c, seen(dx)],
                    moe_x,
                    (dx - 1, o),
                    at(i, dx),
                    tp,
                    (nx - dx - 1, o),
                )
                for o in range(n_y)
            ]
        else:
            sent[n] = [
                to(out_z.at[n], g_moe.at[tp, seen(dx)], moe_a, (n,), at(i, dx), tp, (seen(dx),))
            ]

    def gone(i, dx):
        for copy in sent[i * nx + dx]:
            copy.wait_send()
            sends[:] = [other for other in sends if other is not copy]

    side = range(1, nx)
    wave = [(0, dx) for dx in side] + [(i, 0) for i in range(1, nz)]
    later = [(i, dx) for i in range(1, nz) for dx in side]
    with S("gather_a"):
        for pair in wave[:2]:
            gather(*pair)
    with S("barrier"):
        pl.semaphore_wait(barrier, n_ep + n_tp - 2)
    for pair in wave[:2]:
        send(*pair)
    with S("gather_b"):
        for pair in wave[2:]:
            gather(*pair)
            send(*pair)
    with S("gather_own"):
        for t in range(n_tp):
            g_moe[t, slot(0, 0)] = rows_for(me, slice(t * columns, (t + 1) * columns))
    with S("gather_c"):
        for pair in later:
            gather(*pair)
            send(*pair)

    with S("prep"):
        half = ROPE // 2
        pos = (me * row_count + lax.broadcasted_iota(jnp.int32, (half, row_count), 1)).astype(f32)
        band = lax.broadcasted_iota(jnp.int32, (half, row_count), 0)
        frequency = jnp.zeros((half, row_count), f32)
        for i in range(half):
            frequency = jnp.where(band == i, float(np.float32(frequency_of[i])), frequency)
        angle = pos * frequency
        cosine, sine = jnp.cos(angle), jnp.sin(angle)
        zero = lambda n: jnp.zeros((n, row_count), f32)
        rest = LANES - PLAIN_HEAD_DIM - ROPE
        cos_t = jnp.concatenate(
            [jnp.ones((PLAIN_HEAD_DIM, row_count), f32), cosine, cosine, zero(rest)], axis=0
        ).T
        down_t = jnp.concatenate([zero(PLAIN_HEAD_DIM), -sine, zero(half + rest)], axis=0).T
        up_t = jnp.concatenate([zero(PLAIN_HEAD_DIM + half), sine, zero(rest)], axis=0).T
        shared = rope_ref[...].astype(f32)
        first_half, second_half = shared[:half], shared[half:]
        rope_v[...] = jnp.concatenate(
            [
                zero(PLAIN_HEAD_DIM),
                first_half * cosine - second_half * sine,
                second_half * cosine + first_half * sine,
                zero(rest),
            ],
            axis=0,
        )
        own_lat = my_c * nx
        loads[1].wait()
        c = ckv_v[...].astype(f32)
        level = lax.rsqrt(jnp.mean(c * c, axis=-1, keepdims=True) + EPSILON)
        own_block = g_lat.at[own_lat, my_z]
        own_block[:, :latent] = (c * level * lgain_ref[...]).astype(bf16)
        own_block[:, latent:] = rope_v[:, half_rows].T.astype(bf16)
        loads[2].wait()
        width = PLAIN_HEAD_DIM + ROPE
        for h in range(heads):
            start = (h * width) // LANES * LANES
            shift = h * width - start
            size = LANES if shift + width <= LANES else 2 * LANES
            x = qraw[:, start : start + size].astype(f32)
            if shift:
                x = pltpu.roll(x, size - shift, 1)
            x = x[:, :LANES]
            q_ref[:, h * LANES : (h + 1) * LANES] = (
                x * cos_t + pltpu.roll(x, LANES - half, 1) * down_t + pltpu.roll(x, half, 1) * up_t
            ).astype(bf16)

    lat_over, lat_side = {}, {}

    def lat_hop(d):
        if d == 0:
            src = g_lat.at[own_lat, my_z]

            @pl.when(my_z + 1 < nz)
            def _():
                remote(src, src, lat_up, (my_z,), (my_z,), me + nx, tp).start()

            @pl.when(my_z > 0)
            def _():
                remote(src, src, lat_dn, (my_z,), (my_z,), me - nx, tp).start()

            lat_share(my_z)
        else:
            @pl.when(my_z >= d)
            def _():
                z = my_z - d
                src = g_lat.at[own_lat, z]
                come(src, lat_up, (z,))

                @pl.when(my_z + 1 < nz)
                def _():
                    remote(src, src, lat_up, (z,), (z,), me + nx, tp).start()

                lat_share(z)

            @pl.when(my_z + d < nz)
            def _():
                z = my_z + d
                src = g_lat.at[own_lat, z]
                come(src, lat_dn, (z,))

                @pl.when(my_z > 0)
                def _():
                    remote(src, src, lat_dn, (z,), (z,), me - nx, tp).start()

                lat_share(z)

    def lat_share(z):
        mine = g_lat.at[own_lat, z]
        remote(mine, mine, lat_c, (0, z), (0, z), me, mate).start()
        if nx > 1:
            side = g_lat.at[own_lat + 1, z]
            remote(mine, side, lat_x, (z,), (z,), my_z * nx + 1 - my_x, tp).start()

    def lat_cross(z):
        if nx > 1:
            side = g_lat.at[own_lat + 1, z]
            come(side, lat_x, (z,))
            remote(side, side, lat_c, (1, z), (1, z), me, mate).start()

    def lat_done(z):
        for i in range(nx):
            come(g_lat.at[(1 - my_c) * nx + i, z], lat_c, (i, z))

    def lat_drain():
        for z in range(nz):
            block = g_lat.at[own_lat, z]

            @pl.when(jnp.logical_and(my_z >= z, my_z + 1 < nz))
            def _():
                remote(block, block, lat_up, (z,), (z,), me, mate).wait_send()

            @pl.when(jnp.logical_and(my_z <= z, my_z > 0))
            def _():
                remote(block, block, lat_dn, (z,), (z,), me, mate).wait_send()

            remote(block, block, lat_c, (0, z), (0, z), me, mate).wait_send()
            if nx > 1:
                side = g_lat.at[own_lat + 1, z]
                remote(block, block, lat_x, (z,), (z,), me, mate).wait_send()
                remote(side, side, lat_c, (1, z), (1, z), me, mate).wait_send()

    relay_y, relay_c = {}, {}

    def arrive(i, dx):
        relay_c[i, dx] = []
        for o in range(n_y):
            block = g_moe.at[o * CORES + my_c, slot(i, dx)]
            come(block, moe_x, (dx - 1, o))
            relay_c[i, dx].append(to(block, block, moe_xc, (dx - 1, o), me, mate))

    def spread(i, dx, when=None):
        n = i * nx + dx
        block = g_moe.at[tp, slot(i, dx)]
        copies = []
        for o in range(1, n_y):
            other = lax.rem(my_y + o, n_y) * CORES + my_c
            relay_y[n, o] = remote(block, block, moe_y, (o - 1, n - nx), (o - 1, n - nx), me, other)
            copies.append(relay_y[n, o])
        relay_c[i, dx] = [remote(block, block, moe_c, (0, n - nx), (0, n - nx), me, mate)]
        copies += relay_c[i, dx]

        def run():
            come(block, moe_a, (slot(i, dx),))
            for copy in copies:
                copy.start()

        if when is None:
            run()
            sends.extend(copies)
        else:
            pl.when(when)(run)
            if (i, dx) not in spread_once:
                spread_once.add((i, dx))
                sends.extend(copies)

    spread_once = set()
    inner = jnp.logical_and(my_z > 0, my_z + 1 < nz)
    outer = jnp.logical_not(inner)

    def forward(i, dx):
        n = i * nx + dx
        for o in range(1, n_y):
            relay_y[n, o].wait_recv()
            came = g_moe.at[lax.rem(my_y + n_y - o, n_y) * CORES + my_c, slot(i, dx)]
            relay_c[i, dx].append(to(came, came, moe_c, (o, n - nx), me, mate))

    def finish(i):
        for dx in range(nx):
            for copy in relay_c.get((i, dx), ()):
                copy.wait_recv()

    units = [(0, (dx,)) for dx in range(nx)] + [(c, tuple(range(nx))) for c in range(1, nz)]

    def up(u, f):
        c, dxs = units[u]
        span = slice(f * tile, (f + 1) * tile)
        rows = len(dxs) * cap
        gate = jnp.zeros((rows, tile), f32)
        lift = jnp.zeros((rows, tile), f32)
        for t in range(n_tp):
            x = merge_rows(g_moe[t, pl.ds(slot(c, dxs[0]), len(dxs))])
            gate += jnp.dot(
                x, wg[t * columns : (t + 1) * columns, span], preferred_element_type=f32
            )
            lift += jnp.dot(
                x, wu[t * columns : (t + 1) * columns, span], preferred_element_type=f32
            )
        hidden[:rows, span] = (gate / (1.0 + jnp.exp(-gate)) * lift).astype(bf16)

    reduce_c, reduce_y = {}, {}

    def down(u):
        c, dxs = units[u]
        n = c * nx + dxs[0]
        group = slice(n, n + len(dxs))
        span = pl.ds(n, len(dxs))
        for o in list(range(1, n_y)) + [0]:
            y = lax.rem(my_y + o, n_y)
            for mine in range(2):
                t = y * CORES + (my_c if mine else 1 - my_c)
                part[t, group] = (
                    jnp.dot(
                        hidden[: len(dxs) * cap],
                        wd[:, lane_block(t)],
                        preferred_element_type=f32,
                    )
                    .astype(bf16)
                    .reshape(len(dxs), cap, columns)
                )
                if not mine:
                    reduce_c[u, o] = to(part.at[t, span], r1.at[o, span], red_c, (o, u), me, mate)

    def level_two(u):
        c, dxs = units[u]
        for o in range(1, n_y):
            y = lax.rem(my_y + o, n_y)
            reduce_c[u, o].wait_recv()
            for dx in dxs:
                n = c * nx + dx
                s2[o, n] = (
                    part[y * CORES + my_c, n].astype(f32) + r1[o, n].astype(f32)
                ).astype(bf16)
                reduce_y[n, o] = to(
                    s2.at[o, n], r2.at[o, n], red_y, (o - 1, n), me, y * CORES + my_c
                )

    def give_back(u):
        c, dxs = units[u]
        reduce_c[u, 0].wait_recv()
        for dx in dxs:
            n = c * nx + dx
            total = part[tp, n].astype(f32) + r1[0, n].astype(f32)
            for o in range(1, n_y):
                reduce_y[n, o].wait_recv()
                total += r2[o, n].astype(f32)
            tot[n] = total.astype(bf16)
            if n > 0:
                to(tot.at[n], back.at[seen(dx)], ret_a, (n,), at(c, dx), tp, (seen(dx),))

    def combine(i, dx):
        if i == 0 and dx == 0:
            came = tot[0]
        else:
            come(back.at[slot(i, dx)], ret_a, (slot(i, dx),))
            came = back[slot(i, dx)]
        e = at(i, dx)
        weight = jnp.where(chosen(e), mix_ref[pl.ds(e, 1), :], 0.0)
        high = weight.astype(bf16)
        low = (weight - high.astype(f32)).astype(bf16)
        add = lax.dot_general(
            jnp.concatenate([high, low], axis=0),
            jnp.concatenate([came, came], axis=0),
            (((0,), (0,)), ((), ())),
            preferred_element_type=f32,
        )
        if i == 0 and dx == 0:
            acc[...] = add
        else:
            acc[...] += add

    block = nz * share

    def expand(t, carry):
        kv[pl.ds(pl.multiple_of(t * block, block), block), :] = jnp.dot(
            merge_rows(g_lat[t])[:, :latent], wkv_ref[...], preferred_element_type=f32
        ).astype(bf16)
        return carry

    whole_lat = g_lat.reshape(g_lat.shape[0] * block, g_lat.shape[3])
    lane = lax.broadcasted_iota(jnp.int32, (1, LANES), 1)
    packed = 2 if heads % 2 == 0 else 1
    parts = heads // packed
    att_in, att_mate = [], []

    def attend(part_index):
        for h in range(part_index * packed, (part_index + 1) * packed):
            head = kv[:, h * LANES : (h + 1) * LANES]
            keys = jnp.where(lane < PLAIN_HEAD_DIM, head, whole_lat[:, latent : latent + LANES])
            scores = (
                lax.dot_general(
                    q_ref[:, h * LANES : (h + 1) * LANES],
                    keys,
                    (((1,), (1,)), ((), ())),
                    preferred_element_type=f32,
                )
                * scale
            )
            peak = jnp.max(scores, axis=-1, keepdims=True)
            e = jnp.exp(scores - peak)
            total = jnp.sum(e, axis=-1, keepdims=True)
            mixed = jnp.dot(e.astype(bf16), head, preferred_element_type=f32) / total
            if packed == 1:
                mixed = jnp.where(lane < PLAIN_HEAD_DIM, 0.0, mixed)
            elif h % 2 == 0:
                held = pltpu.roll(mixed, VALUE_HEAD_DIM, 1)
            else:
                mixed = jnp.where(lane < VALUE_HEAD_DIM, held, mixed)
        g_att[tp, part_index] = mixed.astype(bf16)

    def att_send(p):
        own = g_att.at[tp, p]
        for o in range(1, n_y):
            other = lax.rem(my_y + o, n_y) * CORES + my_c
            att_in.append((p, o, to(own, own, att_y, (o - 1, p), me, other)))
        att_mate.append(to(own, own, att_c, (0, p), me, mate))

    def att_forward(part_index):
        for p, o, copy in att_in:
            if p == part_index:
                copy.wait_recv()
                came = g_att.at[lax.rem(my_y + n_y - o, n_y) * CORES + my_c, p]
                att_mate.append(to(came, came, att_c, (o, p), me, mate))

    att_copy = pltpu.make_async_copy(att_v, att_dst, in_sem.at[13])
    exp_copy = pltpu.make_async_copy(exp_v, exp_dst, in_sem.at[14])

    def project():
        for copy in att_mate:
            copy.wait_recv()
        total = jnp.zeros(att_v.shape, f32)
        for t in range(n_tp):
            x = jnp.concatenate([g_att[t, p] for p in range(g_att.shape[1])], axis=1)
            width = x.shape[1]
            total += jnp.dot(x, wo_ref[t * width : (t + 1) * width, :], preferred_element_type=f32)
        att_v[...] = total.astype(bf16)
        att_copy.start()

    def weights_in():
        for copy in loads[3:]:
            copy.wait()

    def each(name, f, i, some=range(nx)):
        for dx in some:
            scoped("%s%d%d" % (name, i, dx), f, i, dx)

    def half_up(u, k):
        for f in range(tiles):
            if (2 * f) // tiles == k:
                scoped("up%d_%d" % (u, f), up, u, f)

    last = nz - 1
    first = nx - 1
    scoped("weights", weights_in)
    half_up(0, 0)
    if nz > 1:
        each("spread", spread, 1, range(1))
    half_up(0, 1)
    scoped("down0", down, 0)
    each("arrive", arrive, 0, side)
    scoped("level_two0", level_two, 0)
    scoped("finish0", finish, 0)
    for u in range(1, nx):
        half_up(u, 0)
        if nz > 1 and u == 1:
            each("spread", spread, 1, side)
        half_up(u, 1)
        scoped("down%d" % u, down, u)
    if nz > 1:
        each("forward", forward, 1, range(1))
    if nz > 2:
        for dx in range(nx):
            scoped("ispread2%d" % dx, spread, 2, dx, inner)
    for u in range(1, nx):
        scoped("level_two%d" % u, level_two, u)
    scoped("lat0", lat_hop, 0)
    if nz > 1:
        each("forward", forward, 1, side)
        scoped("finish1", finish, 1)
        half_up(first + 1, 0)
    if nz > 2:
        for dx in range(nx):
            scoped("ospread2%d" % dx, spread, 2, dx, outer)
    for i in range(3, nz):
        each("spread", spread, i)
    if nz > 1:
        half_up(first + 1, 1)
        scoped("down%d" % (first + 1), down, first + 1)
        scoped("lat1", lat_hop, 1)
        if nz > 2:
            each("forward", forward, 2)
    for c in range(2, nz):
        u = first + c
        scoped("finish%d" % c, finish, c)
        scoped("level_two%d" % (u - 1), level_two, u - 1)
        half_up(u, 0)
        if c + 1 < nz:
            each("forward", forward, c + 1, range(1))
        if c == 2:
            for v in range(nx):
                scoped("give_back%d" % v, give_back, v)
        else:
            scoped("give_back%d" % (u - 2), give_back, u - 2)
        scoped("lat%d" % c, lat_hop, c)
        half_up(u, 1)
        if c + 1 < nz:
            each("forward", forward, c + 1, side)
        scoped("down%d" % u, down, u)
    final = len(units) - 1
    scoped("level_two%d" % final, level_two, final)
    if nz > 1:
        scoped("give_back%d" % (final - 1), give_back, final - 1)
    if nz == 2:
        for v in range(nx):
            scoped("give_back%d" % v, give_back, v)
    for z in range(nz):
        scoped("cross%d" % z, lat_cross, z)
    each("combine", combine, 0)
    for z in range(nz):
        scoped("lat_done%d" % z, lat_done, z)
    with S("expand"):
        lax.fori_loop(0, g_lat.shape[0], expand, 0)
    for p in range(parts):
        scoped("attend%d" % p, attend, p)
        att_send(p)
        if p == 0:
            scoped("give_back%d" % final, give_back, final)
    for p in range(parts):
        scoped("att_forward%d" % p, att_forward, p)
    scoped("project", project)
    for i in range(1, nz):
        each("combine", combine, i)
    exp_v[...] = acc[...].astype(bf16)
    exp_copy.start()
    with S("sendwait"):
        for copy in sends:
            copy.wait_send()
    with S("latdrain"):
        lat_drain()
    with S("outwait"):
        att_copy.wait()
        exp_copy.wait()


def local(
    queries,
    compressed_key_value,
    rope_key,
    latent_norm_gain,
    latent_to_key_value,
    out_proj,
    moe_input,
    moe_gain,
    routes,
    route_weight,
    gate_weight,
    up_weight,
    down_weight,
):
    n_ep = lax.axis_size("ep")
    n_tp = lax.axis_size("tp")
    n_y = n_tp // CORES
    bf16 = jnp.bfloat16
    row_count = queries.shape[0]
    heads = latent_to_key_value.shape[1] // (PLAIN_HEAD_DIM + VALUE_HEAD_DIM)
    latent = compressed_key_value.shape[1]
    share = row_count // CORES
    nx, nz = ep_shape(n_ep)
    over = -queries.shape[1] % LANES
    if over:
        queries = jnp.pad(queries, ((0, 0), (0, over)))
    if heads % 2 == 0:
        wo = out_proj
        parts = heads // 2
    else:
        wo = out_proj.reshape(n_tp * heads, VALUE_HEAD_DIM, out_proj.shape[1])
        wo = jnp.concatenate([jnp.zeros_like(wo), wo], axis=1)
        wo = wo.reshape(n_tp * heads * LANES, out_proj.shape[1])
        parts = heads
    model_width = moe_input.shape[1]
    top = routes.shape[1]
    capacity = 3 * row_count // n_ep
    places = -(-capacity // 16) * 16
    columns = model_width // n_tp
    ff = gate_weight.shape[2]
    anywhere = pl.BlockSpec(memory_space=pl.ANY)
    hbm = pl.BlockSpec(memory_space=pltpu.HBM)
    dma = lambda *shape: pltpu.SemaphoreType.DMA((2,) + shape)
    attention, experts = pl.pallas_call(
        functools.partial(fused, n_ep, n_tp, heads, (PLAIN_HEAD_DIM + ROPE) ** (-0.5)),
        out_shape=(
            pltpu.VMEM((row_count, out_proj.shape[1]), bf16),
            pltpu.VMEM((row_count, columns), bf16),
        ),
        in_specs=[hbm] * 13,
        out_specs=(anywhere, anywhere),
        scratch_shapes=[
            pltpu.VMEM((top, row_count), jnp.int32),
            pltpu.VMEM((top, row_count), jnp.float32),
            pltpu.VMEM((1, model_width), jnp.float32),
            pltpu.VMEM((1, latent), jnp.float32),
            pltpu.VMEM((ROPE, row_count), bf16),
            pltpu.VMEM((row_count, model_width), bf16),
            pltpu.VMEM((share, latent), bf16),
            pltpu.VMEM(queries.shape, bf16),
            pltpu.VMEM(latent_to_key_value.shape, bf16),
            pltpu.VMEM(wo.shape, bf16),
            pltpu.VMEM((model_width, ff), bf16),
            pltpu.VMEM((model_width, ff), bf16),
            pltpu.VMEM((ff, model_width), bf16),
            pltpu.VMEM((row_count, model_width), bf16),
            pltpu.VMEM((n_ep, row_count), jnp.int32),
            pltpu.VMEM((n_ep, row_count), jnp.float32),
            pltpu.VMEM((n_ep, places, columns), bf16),
            pltpu.VMEM((nx, n_y, places, columns), bf16),
            pltpu.VMEM((LANES, row_count), jnp.float32),
            pltpu.VMEM((row_count, heads * LANES), bf16),
            pltpu.VMEM((CORES * nx, nz, share, latent + LANES), bf16),
            pltpu.VMEM((n_tp, n_ep, places, columns), bf16),
            pltpu.VMEM((n_tp, parts, row_count, LANES), bf16),
            pltpu.VMEM((n_ep * row_count, heads * LANES), bf16),
            pltpu.VMEM((nx * places, ff), bf16),
            pltpu.VMEM((n_tp, n_ep, places, columns), bf16),
            pltpu.VMEM((n_y, n_ep, places, columns), bf16),
            pltpu.VMEM((n_y, n_ep, places, columns), bf16),
            pltpu.VMEM((n_y, n_ep, places, columns), bf16),
            pltpu.VMEM((n_ep, places, columns), bf16),
            pltpu.VMEM((n_ep, places, columns), bf16),
            pltpu.VMEM((row_count, columns), jnp.float32),
            pltpu.VMEM((row_count, out_proj.shape[1]), bf16),
            pltpu.VMEM((row_count, columns), bf16),
            pltpu.SemaphoreType.DMA((15,)),
            dma(nz),
            dma(nz),
            dma(nz),
            dma(nx, nz),
            dma(n_ep),
            dma(max(nx - 1, 1), n_y),
            dma(max(nx - 1, 1), n_y),
            dma(max(n_y - 1, 1), max(n_ep - nx, 1)),
            dma(n_y, max(n_ep - nx, 1)),
            dma(max(n_y - 1, 1), parts),
            dma(n_y, parts),
            dma(n_y, nx + nz - 1),
            dma(max(n_y - 1, 1), n_ep),
            dma(n_ep),
        ],
        compiler_params=pltpu.CompilerParams(
            collective_id=0, has_side_effects=True, vmem_limit_bytes=60 * 1024 * 1024
        ),
        name="fused",
    )(
        routes.T,
        route_weight.T,
        moe_gain.reshape(1, model_width),
        latent_norm_gain.reshape(1, latent),
        rope_key.T,
        moe_input,
        compressed_key_value,
        queries,
        latent_to_key_value,
        wo,
        gate_weight.reshape(model_width, ff),
        up_weight.reshape(model_width, ff),
        down_weight.reshape(ff, model_width),
    )
    return attention, experts


def solution(mesh):
    return jax.shard_map(
        local,
        mesh=mesh,
        in_specs=(
            P("ep", "tp"),
            P("ep", None),
            P("ep", None),
            P(),
            P(None, "tp"),
            P(None, "tp"),
            P("ep", None),
            P(),
            P("ep", None),
            P("ep", None),
            P("ep", None, "tp"),
            P("ep", None, "tp"),
            P("ep", "tp", None),
        ),
        out_specs=(P("ep", "tp"), P("ep", "tp")),
        check_vma=False,
    )
```

```python
import functools

import jax
import jax.numpy as jnp
import numpy as np
from jax import lax
from jax.experimental import pallas as pl
from jax.experimental.pallas import tpu as pltpu
from jax.sharding import PartitionSpec as P

PLAIN_HEAD_DIM = 64
ROPE = 32
VALUE_HEAD_DIM = 64
LANES = 128
CORES = 2


EPSILON = 1e-06
ROPE_BASE_VALUE = 10000.0


def ep_shape(n_ep):
    nx = 2 if n_ep % 2 == 0 else 1
    return nx, n_ep // nx


def partners(nz):
    side = lambda z: 2 * z < nz
    return [
        sorted(
            (o for o in range(nz) if o != z),
            key=lambda o: (abs(o - z), side(o) != side(z), o),
        )
        for z in range(nz)
    ]


def merge_rows(block):
    return block.reshape(block.shape[0] * block.shape[1], block.shape[2])


def fused(
    n_ep,
    n_tp,
    heads,
    scale,
    routes_hbm,
    weight_hbm,
    mgain_hbm,
    lgain_hbm,
    rope_hbm,
    moe_hbm,
    ckv_hbm,
    q_hbm,
    wkv_hbm,
    wo_hbm,
    wg_hbm,
    wu_hbm,
    wd_hbm,
    att_dst,
    exp_dst,
    routes_ref,
    weight_ref,
    mgain_ref,
    lgain_ref,
    rope_ref,
    moe_v,
    ckv_v,
    qraw,
    wkv_ref,
    wo_ref,
    wg,
    wu,
    wd,
    normed,
    key_ref,
    mix_ref,
    out_z,
    out_x,
    rope_v,
    q_ref,
    g_lat,
    g_moe,
    g_att,
    kv,
    hidden,
    part,
    r1,
    s2,
    r2,
    tot,
    back,
    acc,
    att_v,
    exp_v,
    in_sem,
    lat_up,
    lat_dn,
    lat_x,
    lat_c,
    moe_a,
    moe_x,
    moe_xc,
    moe_y,
    moe_c,
    att_y,
    att_c,
    red_c,
    red_y,
    ret_a,
):
    f32, bf16 = jnp.float32, jnp.bfloat16
    frequency_of = ROPE_BASE_VALUE ** (-np.arange(ROPE // 2, dtype=np.float32) * 2.0 / ROPE)
    me = lax.axis_index("ep")
    tp = lax.axis_index("tp")
    n_y = n_tp // CORES
    my_y = tp // CORES
    my_c = lax.rem(tp, CORES)
    mate = my_y * CORES + (1 - my_c)
    nx, nz = ep_shape(n_ep)
    my_z = me // nx
    my_x = lax.rem(me, nx)
    row_count, model_width = moe_v.shape
    columns = model_width // n_tp
    cap = g_moe.shape[2]
    chunks = nz
    rows = nx * cap
    ff = wg.shape[1]
    tile = min(512, ff)
    tiles = ff // tile
    share = ckv_v.shape[0]
    latent = ckv_v.shape[1]
    sends = []

    zs = [my_z]
    for i in range(nz - 1):
        value = jnp.int32(0)
        for z, others in enumerate(partners(nz)):
            value = jnp.where(my_z == z, others[i], value)
        zs.append(value)

    def slot(i, dx):
        return zs[i] * nx + dx

    def at(i, dx):
        return zs[i] * nx + lax.rem(my_x + dx, nx)

    def seen(dx):
        return my_z * nx + (nx - dx) % nx

    def remote(src, dst, sems, sent, got, ep_id, tp_id):
        return pltpu.make_async_remote_copy(
            src_ref=src,
            dst_ref=dst,
            send_sem=sems.at[(0,) + sent],
            recv_sem=sems.at[(1,) + got],
            device_id=(ep_id, tp_id),
            device_id_type=pl.DeviceIdType.MESH,
        )

    def to(src, dst, sems, index, ep_id, tp_id, got=None):
        copy = remote(src, dst, sems, index, index if got is None else got, ep_id, tp_id)
        copy.start()
        sends.append(copy)
        return copy

    def come(dst, sems, got):
        remote(dst, dst, sems, got, got, me, mate).wait_recv()

    def lane_block(t):
        return pl.ds(pl.multiple_of(t * columns, columns), columns)

    class S:
        def __init__(self, name):
            self.scope = jax.named_scope(name)

        def __enter__(self):
            pl.delay(1)
            self.scope.__enter__()

        def __exit__(self, *args):
            self.scope.__exit__(*args)

    def scoped(name, f, *a):
        with S(name):
            f(*a)

    barrier = pltpu.get_barrier_semaphore()
    for d in range(1, n_ep):
        pl.semaphore_signal(
            barrier,
            inc=1,
            device_id=(lax.rem(me + d, n_ep), tp),
            device_id_type=pl.DeviceIdType.MESH,
        )
    for d in range(1, n_tp):
        pl.semaphore_signal(
            barrier,
            inc=1,
            device_id=(me, lax.rem(tp + d, n_tp)),
            device_id_type=pl.DeviceIdType.MESH,
        )

    loads = []
    small = []
    for i, (source, target) in enumerate(
        (
            (routes_hbm, routes_ref),
            (weight_hbm, weight_ref),
            (mgain_hbm, mgain_ref),
            (lgain_hbm, lgain_ref),
            (rope_hbm, rope_ref),
        )
    ):
        copy = pltpu.make_async_copy(source, target, in_sem.at[8 + i])
        copy.start()
        small.append(copy)
    half_rows = pl.ds(pl.multiple_of(my_c * share, share), share)
    for i, (source, target) in enumerate(
        (
            (moe_hbm, moe_v),
            (ckv_hbm.at[half_rows], ckv_v),
            (q_hbm, qraw),
            (wg_hbm, wg),
            (wu_hbm, wu),
            (wd_hbm, wd),
            (wkv_hbm, wkv_ref),
            (wo_hbm, wo_ref),
        )
    ):
        copy = pltpu.make_async_copy(source, target, in_sem.at[i])
        loads.append(copy)
    loads[0].start()

    with S("routing"):
        for copy in small[:2]:
            copy.wait()
        top = routes_ref.shape[0]
        expert_of = lax.broadcasted_iota(jnp.int32, (n_ep, row_count), 0)
        named = jnp.zeros((n_ep, row_count), f32)
        mix = jnp.zeros((n_ep, row_count), f32)
        for k in range(top):
            hit = routes_ref[k : k + 1, :] == expert_of
            named = jnp.where(hit, 1.0, named)
            mix = jnp.where(hit, weight_ref[k : k + 1, :], mix)
        mix_ref[...] = mix
        first = lax.broadcasted_iota(jnp.int32, (row_count, row_count), 0)
        second = lax.broadcasted_iota(jnp.int32, (row_count, row_count), 1)
        before = jnp.where(first < second, 1.0, 0.0).astype(bf16)
        earlier = jnp.dot(named.astype(bf16), before, preferred_element_type=f32)
        key_ref[...] = jnp.where(named > 0.5, earlier, -1.0).astype(jnp.int32)
    place = lax.broadcasted_iota(jnp.int32, (cap, row_count), 0)

    def chosen(e):
        return key_ref[pl.ds(e, 1), :] == place

    def rows_for(e, cols):
        pick = jnp.where(chosen(e), 1.0, 0.0).astype(bf16)
        return jnp.dot(pick, normed[:, cols], preferred_element_type=f32).astype(bf16)

    with S("norm"):
        loads[0].wait()
        for copy in small[2:]:
            copy.wait()
        for copy in loads[1:]:
            copy.start()
        step_rows = 16

        def norm(i, carry):
            span = pl.ds(pl.multiple_of(i * step_rows, step_rows), step_rows)
            x = moe_v[span, :].astype(f32)
            level = lax.rsqrt(jnp.mean(x * x, axis=-1, keepdims=True) + EPSILON)
            normed[span, :] = (x * level * mgain_ref[...]).astype(bf16)
            return carry

        lax.fori_loop(0, row_count // step_rows, norm, 0, unroll=4)


    def direct(i, dx):
        return i == 0

    sent = {}

    def gather(i, dx):
        n = i * nx + dx
        if direct(i, dx):
            for o in range(n_y):
                out_x[n, o] = rows_for(at(i, dx), lane_block(o * CORES + my_c))
        else:
            out_z[n] = rows_for(at(i, dx), lane_block(tp))

    def send(i, dx):
        n = i * nx + dx
        if direct(i, dx):
            sent[n] = [
                to(
                    out_x.at[n, o],
                    g_moe.at[o * CORES + my_c, seen(dx)],
                    moe_x,
                    (dx - 1, o),
                    at(i, dx),
                    tp,
                    (nx - dx - 1, o),
                )
                for o in range(n_y)
            ]
        else:
            sent[n] = [
                to(out_z.at[n], g_moe.at[tp, seen(dx)], moe_a, (n,), at(i, dx), tp, (seen(dx),))
            ]

    def gone(i, dx):
        for copy in sent[i * nx + dx]:
            copy.wait_send()
            sends[:] = [other for other in sends if other is not copy]

    side = range(1, nx)
    wave = [(0, dx) for dx in side] + [(i, 0) for i in range(1, min(3, nz))]
    later = [(i, dx) for i in (2, 1) for dx in side if i < nz]
    latest = [(i, dx) for i in range(3, nz) for dx in range(nx)]
    with S("gather_a"):
        for pair in wave[:2]:
            gather(*pair)
    with S("barrier"):
        pl.semaphore_wait(barrier, n_ep + n_tp - 2)
    for pair in wave[:2]:
        send(*pair)
    with S("gather_b"):
        for pair in wave[2:]:
            gather(*pair)
            send(*pair)
    with S("gather_own"):
        for t in range(n_tp):
            g_moe[t, slot(0, 0)] = rows_for(me, slice(t * columns, (t + 1) * columns))
    with S("gather_c"):
        for pair in later:
            gather(*pair)
            send(*pair)
        for pair in latest:
            gather(*pair)

    with S("prep"):
        half = ROPE // 2
        pos = (me * row_count + lax.broadcasted_iota(jnp.int32, (half, row_count), 1)).astype(f32)
        band = lax.broadcasted_iota(jnp.int32, (half, row_count), 0)
        frequency = jnp.zeros((half, row_count), f32)
        for i in range(half):
            frequency = jnp.where(band == i, float(np.float32(frequency_of[i])), frequency)
        angle = pos * frequency
        cosine, sine = jnp.cos(angle), jnp.sin(angle)
        zero = lambda n: jnp.zeros((n, row_count), f32)
        rest = LANES - PLAIN_HEAD_DIM - ROPE
        cos_t = jnp.concatenate(
            [jnp.ones((PLAIN_HEAD_DIM, row_count), f32), cosine, cosine, zero(rest)], axis=0
        ).T
        down_t = jnp.concatenate([zero(PLAIN_HEAD_DIM), -sine, zero(half + rest)], axis=0).T
        up_t = jnp.concatenate([zero(PLAIN_HEAD_DIM + half), sine, zero(rest)], axis=0).T
        shared = rope_ref[...].astype(f32)
        first_half, second_half = shared[:half], shared[half:]
        rope_v[...] = jnp.concatenate(
            [
                zero(PLAIN_HEAD_DIM),
                first_half * cosine - second_half * sine,
                second_half * cosine + first_half * sine,
                zero(rest),
            ],
            axis=0,
        )
        own_lat = my_c * nx
        loads[1].wait()
        c = ckv_v[...].astype(f32)
        level = lax.rsqrt(jnp.mean(c * c, axis=-1, keepdims=True) + EPSILON)
        own_block = g_lat.at[own_lat, my_z]
        own_block[:, :latent] = (c * level * lgain_ref[...]).astype(bf16)
        own_block[:, latent:] = rope_v[:, half_rows].T.astype(bf16)
        loads[2].wait()
        width = PLAIN_HEAD_DIM + ROPE
        for h in range(heads):
            start = (h * width) // LANES * LANES
            shift = h * width - start
            size = LANES if shift + width <= LANES else 2 * LANES
            x = qraw[:, start : start + size].astype(f32)
            if shift:
                x = pltpu.roll(x, size - shift, 1)
            x = x[:, :LANES]
            q_ref[:, h * LANES : (h + 1) * LANES] = (
                x * cos_t + pltpu.roll(x, LANES - half, 1) * down_t + pltpu.roll(x, half, 1) * up_t
            ).astype(bf16)

    lat_over, lat_side = {}, {}

    def lat_hop(d):
        if d == 0:
            src = g_lat.at[own_lat, my_z]

            @pl.when(my_z + 1 < nz)
            def _():
                remote(src, src, lat_up, (my_z,), (my_z,), me + nx, tp).start()

            @pl.when(my_z > 0)
            def _():
                remote(src, src, lat_dn, (my_z,), (my_z,), me - nx, tp).start()

            lat_share(my_z)
        else:
            @pl.when(my_z >= d)
            def _():
                z = my_z - d
                src = g_lat.at[own_lat, z]
                come(src, lat_up, (z,))

                @pl.when(my_z + 1 < nz)
                def _():
                    remote(src, src, lat_up, (z,), (z,), me + nx, tp).start()

                lat_share(z)

            @pl.when(my_z + d < nz)
            def _():
                z = my_z + d
                src = g_lat.at[own_lat, z]
                come(src, lat_dn, (z,))

                @pl.when(my_z > 0)
                def _():
                    remote(src, src, lat_dn, (z,), (z,), me - nx, tp).start()

                lat_share(z)

    def lat_share(z):
        mine = g_lat.at[own_lat, z]
        remote(mine, mine, lat_c, (0, z), (0, z), me, mate).start()
        if nx > 1:
            side = g_lat.at[own_lat + 1, z]
            remote(mine, side, lat_x, (z,), (z,), my_z * nx + 1 - my_x, tp).start()

    def lat_cross(z):
        if nx > 1:
            side = g_lat.at[own_lat + 1, z]
            come(side, lat_x, (z,))
            remote(side, side, lat_c, (1, z), (1, z), me, mate).start()

    def lat_done(z):
        for i in range(nx):
            come(g_lat.at[(1 - my_c) * nx + i, z], lat_c, (i, z))

    def lat_drain():
        for z in range(nz):
            block = g_lat.at[own_lat, z]

            @pl.when(jnp.logical_and(my_z >= z, my_z + 1 < nz))
            def _():
                remote(block, block, lat_up, (z,), (z,), me, mate).wait_send()

            @pl.when(jnp.logical_and(my_z <= z, my_z > 0))
            def _():
                remote(block, block, lat_dn, (z,), (z,), me, mate).wait_send()

            remote(block, block, lat_c, (0, z), (0, z), me, mate).wait_send()
            if nx > 1:
                side = g_lat.at[own_lat + 1, z]
                remote(block, block, lat_x, (z,), (z,), me, mate).wait_send()
                remote(side, side, lat_c, (1, z), (1, z), me, mate).wait_send()

    relay_y, relay_c = {}, {}

    def arrive(i, dx):
        relay_c[i, dx] = []
        for o in range(n_y):
            block = g_moe.at[o * CORES + my_c, slot(i, dx)]
            come(block, moe_x, (dx - 1, o))
            relay_c[i, dx].append(to(block, block, moe_xc, (dx - 1, o), me, mate))

    def spread(i, dx, when=None):
        n = i * nx + dx
        block = g_moe.at[tp, slot(i, dx)]
        copies = []
        for o in range(1, n_y):
            other = lax.rem(my_y + o, n_y) * CORES + my_c
            relay_y[n, o] = remote(block, block, moe_y, (o - 1, n - nx), (o - 1, n - nx), me, other)
            copies.append(relay_y[n, o])
        relay_c[i, dx] = [remote(block, block, moe_c, (0, n - nx), (0, n - nx), me, mate)]
        copies += relay_c[i, dx]

        def run():
            come(block, moe_a, (slot(i, dx),))
            for copy in copies:
                copy.start()

        if when is None:
            run()
            sends.extend(copies)
        else:
            pl.when(when)(run)
            if (i, dx) not in spread_once:
                spread_once.add((i, dx))
                sends.extend(copies)

    spread_once = set()
    inner = jnp.logical_and(my_z > 0, my_z + 1 < nz)
    outer = jnp.logical_not(inner)

    def forward(i, dx):
        n = i * nx + dx
        for o in range(1, n_y):
            relay_y[n, o].wait_recv()
            came = g_moe.at[lax.rem(my_y + n_y - o, n_y) * CORES + my_c, slot(i, dx)]
            relay_c[i, dx].append(to(came, came, moe_c, (o, n - nx), me, mate))

    def finish(i):
        for dx in range(nx):
            for copy in relay_c.get((i, dx), ()):
                copy.wait_recv()

    units = [(0, (dx,)) for dx in range(nx)] + [(c, tuple(range(nx))) for c in range(1, nz)]

    def up(u, f):
        c, dxs = units[u]
        span = slice(f * tile, (f + 1) * tile)
        rows = len(dxs) * cap
        gate = jnp.zeros((rows, tile), f32)
        lift = jnp.zeros((rows, tile), f32)
        for t in range(n_tp):
            x = merge_rows(g_moe[t, pl.ds(slot(c, dxs[0]), len(dxs))])
            gate += jnp.dot(
                x, wg[t * columns : (t + 1) * columns, span], preferred_element_type=f32
            )
            lift += jnp.dot(
                x, wu[t * columns : (t + 1) * columns, span], preferred_element_type=f32
            )
        hidden[:rows, span] = (gate / (1.0 + jnp.exp(-gate)) * lift).astype(bf16)

    reduce_c, reduce_y = {}, {}

    def down(u):
        c, dxs = units[u]
        n = c * nx + dxs[0]
        group = slice(n, n + len(dxs))
        span = pl.ds(n, len(dxs))
        for o in list(range(1, n_y)) + [0]:
            y = lax.rem(my_y + o, n_y)
            for mine in range(2):
                t = y * CORES + (my_c if mine else 1 - my_c)
                part[t, group] = (
                    jnp.dot(
                        hidden[: len(dxs) * cap],
                        wd[:, lane_block(t)],
                        preferred_element_type=f32,
                    )
                    .astype(bf16)
                    .reshape(len(dxs), cap, columns)
                )
                if not mine:
                    reduce_c[u, o] = to(part.at[t, span], r1.at[o, span], red_c, (o, u), me, mate)

    def level_two(u):
        c, dxs = units[u]
        for o in range(1, n_y):
            y = lax.rem(my_y + o, n_y)
            reduce_c[u, o].wait_recv()
            for dx in dxs:
                n = c * nx + dx
                s2[o, n] = (
                    part[y * CORES + my_c, n].astype(f32) + r1[o, n].astype(f32)
                ).astype(bf16)
                reduce_y[n, o] = to(
                    s2.at[o, n], r2.at[o, n], red_y, (o - 1, n), me, y * CORES + my_c
                )

    def give_back(u):
        c, dxs = units[u]
        reduce_c[u, 0].wait_recv()
        for dx in dxs:
            n = c * nx + dx
            total = part[tp, n].astype(f32) + r1[0, n].astype(f32)
            for o in range(1, n_y):
                reduce_y[n, o].wait_recv()
                total += r2[o, n].astype(f32)
            tot[n] = total.astype(bf16)
            if n > 0:
                to(tot.at[n], back.at[seen(dx)], ret_a, (n,), at(c, dx), tp, (seen(dx),))

    def combine(i, dx):
        if i == 0 and dx == 0:
            came = tot[0]
        else:
            come(back.at[slot(i, dx)], ret_a, (slot(i, dx),))
            came = back[slot(i, dx)]
        e = at(i, dx)
        weight = jnp.where(chosen(e), mix_ref[pl.ds(e, 1), :], 0.0)
        high = weight.astype(bf16)
        low = (weight - high.astype(f32)).astype(bf16)
        add = lax.dot_general(
            jnp.concatenate([high, low], axis=0),
            jnp.concatenate([came, came], axis=0),
            (((0,), (0,)), ((), ())),
            preferred_element_type=f32,
        )
        if i == 0 and dx == 0:
            acc[...] = add
        else:
            acc[...] += add

    block = nz * share

    def expand(z):
        lat_done(z)
        for t in range(g_lat.shape[0]):
            span = pl.ds(pl.multiple_of(t * block + z * share, share), share)
            kv[span, :] = jnp.dot(
                g_lat[t, z][:, :latent], wkv_ref[...], preferred_element_type=f32
            ).astype(bf16)

    def around(d, f):
        if d == 0:
            f(my_z)
        else:
            pl.when(my_z >= d)(lambda: f(my_z - d))
            pl.when(my_z + d < nz)(lambda: f(my_z + d))

    whole_lat = g_lat.reshape(g_lat.shape[0] * block, g_lat.shape[3])
    lane = lax.broadcasted_iota(jnp.int32, (1, LANES), 1)
    packed = 2 if heads % 2 == 0 else 1
    parts = heads // packed
    att_in, att_mate = [], []

    def attend(part_index):
        for h in range(part_index * packed, (part_index + 1) * packed):
            head = kv[:, h * LANES : (h + 1) * LANES]
            keys = jnp.where(lane < PLAIN_HEAD_DIM, head, whole_lat[:, latent : latent + LANES])
            scores = (
                lax.dot_general(
                    q_ref[:, h * LANES : (h + 1) * LANES],
                    keys,
                    (((1,), (1,)), ((), ())),
                    preferred_element_type=f32,
                )
                * scale
            )
            peak = jnp.max(scores, axis=-1, keepdims=True)
            e = jnp.exp(scores - peak)
            total = jnp.sum(e, axis=-1, keepdims=True)
            mixed = jnp.dot(e.astype(bf16), head, preferred_element_type=f32) / total
            if packed == 1:
                mixed = jnp.where(lane < PLAIN_HEAD_DIM, 0.0, mixed)
            elif h % 2 == 0:
                held = pltpu.roll(mixed, VALUE_HEAD_DIM, 1)
            else:
                mixed = jnp.where(lane < VALUE_HEAD_DIM, held, mixed)
        g_att[tp, part_index] = mixed.astype(bf16)

    def att_send(p):
        own = g_att.at[tp, p]
        for o in range(1, n_y):
            other = lax.rem(my_y + o, n_y) * CORES + my_c
            att_in.append((p, o, to(own, own, att_y, (o - 1, p), me, other)))
        att_mate.append(to(own, own, att_c, (0, p), me, mate))

    def att_forward(part_index):
        for p, o, copy in att_in:
            if p == part_index:
                copy.wait_recv()
                came = g_att.at[lax.rem(my_y + n_y - o, n_y) * CORES + my_c, p]
                att_mate.append(to(came, came, att_c, (o, p), me, mate))

    att_copy = pltpu.make_async_copy(att_v, att_dst, in_sem.at[13])
    exp_copy = pltpu.make_async_copy(exp_v, exp_dst, in_sem.at[14])

    def project():
        for copy in att_mate:
            copy.wait_recv()
        total = jnp.zeros(att_v.shape, f32)
        for t in range(n_tp):
            x = jnp.concatenate([g_att[t, p] for p in range(g_att.shape[1])], axis=1)
            width = x.shape[1]
            total += jnp.dot(x, wo_ref[t * width : (t + 1) * width, :], preferred_element_type=f32)
        att_v[...] = total.astype(bf16)
        att_copy.start()

    def weights_in():
        for copy in loads[3:]:
            copy.wait()

    def each(name, f, i, some=range(nx)):
        for dx in some:
            scoped("%s%d%d" % (name, i, dx), f, i, dx)

    def half_up(u, k):
        with S("up%d_%d" % (u, k)):
            for f in range(tiles):
                if (2 * f) // tiles == k:
                    up(u, f)

    last = nz - 1
    first = nx - 1
    scoped("weights", weights_in)
    for pair in latest:
        send(*pair)
    half_up(0, 0)
    if nz > 1:
        each("spread", spread, 1, range(1))
    half_up(0, 1)
    scoped("down0", down, 0)
    each("arrive", arrive, 0, side)
    scoped("level_two0", level_two, 0)
    scoped("finish0", finish, 0)
    for u in range(1, nx):
        half_up(u, 0)
        if nz > 1 and u == 1:
            for dx in side:
                scoped("ospread1%d" % dx, spread, 1, dx, outer)
        half_up(u, 1)
        scoped("down%d" % u, down, u)
    if nz > 1:
        for dx in side:
            scoped("ispread1%d" % dx, spread, 1, dx, inner)
    if nz > 2:
        scoped("ispread20", spread, 2, 0, inner)
    if nz > 1:
        each("forward", forward, 1, range(1))
    for u in range(1, nx):
        scoped("level_two%d" % u, level_two, u)
    scoped("lat0", lat_hop, 0)
    if nz > 2:
        for dx in side:
            scoped("ispread2%d" % dx, spread, 2, dx, inner)
    if nz > 1:
        each("forward", forward, 1, side)
        scoped("finish1", finish, 1)
        half_up(first + 1, 0)
    if nz > 2:
        for dx in range(nx):
            scoped("ospread2%d" % dx, spread, 2, dx, outer)
    for i in range(3, nz):
        each("spread", spread, i)
    if nz > 1:
        half_up(first + 1, 1)
        scoped("down%d" % (first + 1), down, first + 1)
        scoped("lat1", lat_hop, 1)
        if nz > 2:
            each("forward", forward, 2)
    for c in range(2, nz):
        u = first + c
        scoped("finish%d" % c, finish, c)
        scoped("level_two%d" % (u - 1), level_two, u - 1)
        half_up(u, 0)
        if c + 1 < nz:
            each("forward", forward, c + 1, range(1))
        if c == 2:
            for v in range(nx):
                scoped("give_back%d" % v, give_back, v)
        else:
            scoped("give_back%d" % (u - 2), give_back, u - 2)
        scoped("lat%d" % c, lat_hop, c)
        half_up(u, 1)
        if c + 1 < nz:
            each("forward", forward, c + 1, side)
        scoped("down%d" % u, down, u)
    final = len(units) - 1
    scoped("level_two%d" % final, level_two, final)
    if nz > 1:
        scoped("give_back%d" % (final - 1), give_back, final - 1)
    if nz == 2:
        for v in range(nx):
            scoped("give_back%d" % v, give_back, v)
    for d in range(min(2, nz)):
        scoped("cross%d" % d, around, d, lat_cross)
    scoped("expand0", around, 0, expand)
    for d in range(2, nz):
        if d == last:
            scoped("expand%d" % (d - 2), around, d - 2, expand)
            scoped("expand%d" % (d - 1), around, d - 1, expand)
            scoped("cross%d" % d, around, d, lat_cross)
        else:
            scoped("cross%d" % d, around, d, lat_cross)
            if d > 2:
                scoped("expand%d" % (d - 2), around, d - 2, expand)
    each("combine", combine, 0)
    if nz > 1:
        scoped("expand%d" % last, around, last, expand)
    scoped("give_back%d" % final, give_back, final)
    for p in range(parts):
        scoped("attend%d" % p, attend, p)
        att_send(p)
    for p in range(parts):
        scoped("att_forward%d" % p, att_forward, p)
    scoped("project", project)
    for i in range(1, nz):
        each("combine", combine, i)
    exp_v[...] = acc[...].astype(bf16)
    exp_copy.start()
    with S("sendwait"):
        for copy in sends:
            copy.wait_send()
    with S("latdrain"):
        lat_drain()
    with S("outwait"):
        att_copy.wait()
        exp_copy.wait()


def local(
    queries,
    compressed_key_value,
    rope_key,
    latent_norm_gain,
    latent_to_key_value,
    out_proj,
    moe_input,
    moe_gain,
    routes,
    route_weight,
    gate_weight,
    up_weight,
    down_weight,
):
    n_ep = lax.axis_size("ep")
    n_tp = lax.axis_size("tp")
    n_y = n_tp // CORES
    bf16 = jnp.bfloat16
    row_count = queries.shape[0]
    heads = latent_to_key_value.shape[1] // (PLAIN_HEAD_DIM + VALUE_HEAD_DIM)
    latent = compressed_key_value.shape[1]
    share = row_count // CORES
    nx, nz = ep_shape(n_ep)
    over = -queries.shape[1] % LANES
    if over:
        queries = jnp.pad(queries, ((0, 0), (0, over)))
    if heads % 2 == 0:
        wo = out_proj
        parts = heads // 2
    else:
        wo = out_proj.reshape(n_tp * heads, VALUE_HEAD_DIM, out_proj.shape[1])
        wo = jnp.concatenate([jnp.zeros_like(wo), wo], axis=1)
        wo = wo.reshape(n_tp * heads * LANES, out_proj.shape[1])
        parts = heads
    model_width = moe_input.shape[1]
    top = routes.shape[1]
    capacity = 3 * row_count // n_ep
    places = -(-capacity // 16) * 16
    columns = model_width // n_tp
    ff = gate_weight.shape[2]
    anywhere = pl.BlockSpec(memory_space=pl.ANY)
    hbm = pl.BlockSpec(memory_space=pltpu.HBM)
    dma = lambda *shape: pltpu.SemaphoreType.DMA((2,) + shape)
    attention, experts = pl.pallas_call(
        functools.partial(fused, n_ep, n_tp, heads, (PLAIN_HEAD_DIM + ROPE) ** (-0.5)),
        out_shape=(
            pltpu.VMEM((row_count, out_proj.shape[1]), bf16),
            pltpu.VMEM((row_count, columns), bf16),
        ),
        in_specs=[hbm] * 13,
        out_specs=(anywhere, anywhere),
        scratch_shapes=[
            pltpu.VMEM((top, row_count), jnp.int32),
            pltpu.VMEM((top, row_count), jnp.float32),
            pltpu.VMEM((1, model_width), jnp.float32),
            pltpu.VMEM((1, latent), jnp.float32),
            pltpu.VMEM((ROPE, row_count), bf16),
            pltpu.VMEM((row_count, model_width), bf16),
            pltpu.VMEM((share, latent), bf16),
            pltpu.VMEM(queries.shape, bf16),
            pltpu.VMEM(latent_to_key_value.shape, bf16),
            pltpu.VMEM(wo.shape, bf16),
            pltpu.VMEM((model_width, ff), bf16),
            pltpu.VMEM((model_width, ff), bf16),
            pltpu.VMEM((ff, model_width), bf16),
            pltpu.VMEM((row_count, model_width), bf16),
            pltpu.VMEM((n_ep, row_count), jnp.int32),
            pltpu.VMEM((n_ep, row_count), jnp.float32),
            pltpu.VMEM((n_ep, places, columns), bf16),
            pltpu.VMEM((nx, n_y, places, columns), bf16),
            pltpu.VMEM((LANES, row_count), jnp.float32),
            pltpu.VMEM((row_count, heads * LANES), bf16),
            pltpu.VMEM((CORES * nx, nz, share, latent + LANES), bf16),
            pltpu.VMEM((n_tp, n_ep, places, columns), bf16),
            pltpu.VMEM((n_tp, parts, row_count, LANES), bf16),
            pltpu.VMEM((n_ep * row_count, heads * LANES), bf16),
            pltpu.VMEM((nx * places, ff), bf16),
            pltpu.VMEM((n_tp, n_ep, places, columns), bf16),
            pltpu.VMEM((n_y, n_ep, places, columns), bf16),
            pltpu.VMEM((n_y, n_ep, places, columns), bf16),
            pltpu.VMEM((n_y, n_ep, places, columns), bf16),
            pltpu.VMEM((n_ep, places, columns), bf16),
            pltpu.VMEM((n_ep, places, columns), bf16),
            pltpu.VMEM((row_count, columns), jnp.float32),
            pltpu.VMEM((row_count, out_proj.shape[1]), bf16),
            pltpu.VMEM((row_count, columns), bf16),
            pltpu.SemaphoreType.DMA((15,)),
            dma(nz),
            dma(nz),
            dma(nz),
            dma(nx, nz),
            dma(n_ep),
            dma(max(nx - 1, 1), n_y),
            dma(max(nx - 1, 1), n_y),
            dma(max(n_y - 1, 1), max(n_ep - nx, 1)),
            dma(n_y, max(n_ep - nx, 1)),
            dma(max(n_y - 1, 1), parts),
            dma(n_y, parts),
            dma(n_y, nx + nz - 1),
            dma(max(n_y - 1, 1), n_ep),
            dma(n_ep),
        ],
        compiler_params=pltpu.CompilerParams(
            collective_id=0, has_side_effects=True, vmem_limit_bytes=60 * 1024 * 1024
        ),
        name="fused",
    )(
        routes.T,
        route_weight.T,
        moe_gain.reshape(1, model_width),
        latent_norm_gain.reshape(1, latent),
        rope_key.T,
        moe_input,
        compressed_key_value,
        queries,
        latent_to_key_value,
        wo,
        gate_weight.reshape(model_width, ff),
        up_weight.reshape(model_width, ff),
        down_weight.reshape(ff, model_width),
    )
    return attention, experts


def solution(mesh):
    return jax.shard_map(
        local,
        mesh=mesh,
        in_specs=(
            P("ep", "tp"),
            P("ep", None),
            P("ep", None),
            P(),
            P(None, "tp"),
            P(None, "tp"),
            P("ep", None),
            P(),
            P("ep", None),
            P("ep", None),
            P("ep", None, "tp"),
            P("ep", None, "tp"),
            P("ep", "tp", None),
        ),
        out_specs=(P("ep", "tp"), P("ep", "tp")),
        check_vma=False,
    )
```

```python
import functools

import jax
import jax.numpy as jnp
import numpy as np
from jax import lax
from jax.experimental import pallas as pl
from jax.experimental.pallas import tpu as pltpu
from jax.sharding import PartitionSpec as P

PLAIN_HEAD_DIM = 64
ROPE = 32
VALUE_HEAD_DIM = 64
LANES = 128
CORES = 2


EPSILON = 1e-06
ROPE_BASE_VALUE = 10000.0


def ep_shape(n_ep):
    nx = 2 if n_ep % 2 == 0 else 1
    return nx, n_ep // nx


def partners(nz):
    side = lambda z: 2 * z < nz
    return [
        sorted(
            (o for o in range(nz) if o != z),
            key=lambda o: (abs(o - z), side(o) != side(z), o),
        )
        for z in range(nz)
    ]


def merge_rows(block):
    return block.reshape(block.shape[0] * block.shape[1], block.shape[2])


def fused(
    n_ep,
    n_tp,
    heads,
    scale,
    routes_hbm,
    weight_hbm,
    mgain_hbm,
    lgain_hbm,
    rope_hbm,
    moe_hbm,
    ckv_hbm,
    q_hbm,
    wkv_hbm,
    wo_hbm,
    wg_hbm,
    wu_hbm,
    wd_hbm,
    att_dst,
    exp_dst,
    routes_ref,
    weight_ref,
    mgain_ref,
    lgain_ref,
    rope_ref,
    moe_v,
    ckv_v,
    qraw,
    wkv_ref,
    wo_ref,
    wg,
    wu,
    wd,
    normed,
    key_ref,
    mix_ref,
    out_z,
    out_x,
    rope_v,
    q_ref,
    g_lat,
    g_moe,
    g_att,
    kv,
    hidden,
    part,
    r1,
    s2,
    r2,
    tot,
    back,
    acc,
    att_v,
    exp_v,
    in_sem,
    lat_z,
    lat_x,
    lat_c,
    moe_a,
    moe_x,
    moe_xc,
    moe_y,
    moe_c,
    att_y,
    att_c,
    red_c,
    red_y,
    ret_a,
):
    f32, bf16 = jnp.float32, jnp.bfloat16
    frequency_of = ROPE_BASE_VALUE ** (-np.arange(ROPE // 2, dtype=np.float32) * 2.0 / ROPE)
    me = lax.axis_index("ep")
    tp = lax.axis_index("tp")
    n_y = n_tp // CORES
    my_y = tp // CORES
    my_c = lax.rem(tp, CORES)
    mate = my_y * CORES + (1 - my_c)
    nx, nz = ep_shape(n_ep)
    my_z = me // nx
    my_x = lax.rem(me, nx)
    row_count, model_width = moe_v.shape
    columns = model_width // n_tp
    cap = g_moe.shape[2]
    chunks = nz
    rows = nx * cap
    ff = wg.shape[1]
    tile = min(512, ff)
    tiles = ff // tile
    share = ckv_v.shape[0]
    latent = ckv_v.shape[1]
    sends = []

    zs = [my_z]
    for i in range(nz - 1):
        value = jnp.int32(0)
        for z, others in enumerate(partners(nz)):
            value = jnp.where(my_z == z, others[i], value)
        zs.append(value)

    def slot(i, dx):
        return zs[i] * nx + dx

    def at(i, dx):
        return zs[i] * nx + lax.rem(my_x + dx, nx)

    def seen(dx):
        return my_z * nx + (nx - dx) % nx

    def remote(src, dst, sems, sent, got, ep_id, tp_id):
        return pltpu.make_async_remote_copy(
            src_ref=src,
            dst_ref=dst,
            send_sem=sems.at[(0,) + sent],
            recv_sem=sems.at[(1,) + got],
            device_id=(ep_id, tp_id),
            device_id_type=pl.DeviceIdType.MESH,
        )

    def to(src, dst, sems, index, ep_id, tp_id, got=None):
        copy = remote(src, dst, sems, index, index if got is None else got, ep_id, tp_id)
        copy.start()
        sends.append(copy)
        return copy

    def come(dst, sems, got):
        remote(dst, dst, sems, got, got, me, mate).wait_recv()

    def lane_block(t):
        return pl.ds(pl.multiple_of(t * columns, columns), columns)

    class S:
        def __init__(self, name):
            self.scope = jax.named_scope(name)

        def __enter__(self):
            pl.delay(1)
            self.scope.__enter__()

        def __exit__(self, *args):
            self.scope.__exit__(*args)

    def scoped(name, f, *a):
        with S(name):
            f(*a)

    barrier = pltpu.get_barrier_semaphore()
    for d in range(1, n_ep):
        pl.semaphore_signal(
            barrier,
            inc=1,
            device_id=(lax.rem(me + d, n_ep), tp),
            device_id_type=pl.DeviceIdType.MESH,
        )
    for d in range(1, n_tp):
        pl.semaphore_signal(
            barrier,
            inc=1,
            device_id=(me, lax.rem(tp + d, n_tp)),
            device_id_type=pl.DeviceIdType.MESH,
        )

    loads = []
    small = []
    for i, (source, target) in enumerate(
        (
            (routes_hbm, routes_ref),
            (weight_hbm, weight_ref),
            (mgain_hbm, mgain_ref),
            (lgain_hbm, lgain_ref),
            (rope_hbm, rope_ref),
        )
    ):
        copy = pltpu.make_async_copy(source, target, in_sem.at[8 + i])
        copy.start()
        small.append(copy)
    half_rows = pl.ds(pl.multiple_of(my_c * share, share), share)
    for i, (source, target) in enumerate(
        (
            (moe_hbm, moe_v),
            (ckv_hbm.at[half_rows], ckv_v),
            (q_hbm, qraw),
            (wg_hbm, wg),
            (wu_hbm, wu),
            (wd_hbm, wd),
            (wkv_hbm, wkv_ref),
            (wo_hbm, wo_ref),
        )
    ):
        copy = pltpu.make_async_copy(source, target, in_sem.at[i])
        loads.append(copy)
    loads[0].start()

    with S("routing"):
        for copy in small[:2]:
            copy.wait()
        top = routes_ref.shape[0]
        expert_of = lax.broadcasted_iota(jnp.int32, (n_ep, row_count), 0)
        named = jnp.zeros((n_ep, row_count), f32)
        mix = jnp.zeros((n_ep, row_count), f32)
        for k in range(top):
            hit = routes_ref[k : k + 1, :] == expert_of
            named = jnp.where(hit, 1.0, named)
            mix = jnp.where(hit, weight_ref[k : k + 1, :], mix)
        mix_ref[...] = mix
        first = lax.broadcasted_iota(jnp.int32, (row_count, row_count), 0)
        second = lax.broadcasted_iota(jnp.int32, (row_count, row_count), 1)
        before = jnp.where(first < second, 1.0, 0.0).astype(bf16)
        earlier = jnp.dot(named.astype(bf16), before, preferred_element_type=f32)
        key_ref[...] = jnp.where(named > 0.5, earlier, -1.0).astype(jnp.int32)
    place = lax.broadcasted_iota(jnp.int32, (cap, row_count), 0)

    def chosen(e):
        return key_ref[pl.ds(e, 1), :] == place

    def rows_for(e, cols):
        pick = jnp.where(chosen(e), 1.0, 0.0).astype(bf16)
        return jnp.dot(pick, normed[:, cols], preferred_element_type=f32).astype(bf16)

    with S("norm"):
        loads[0].wait()
        for copy in small[2:]:
            copy.wait()
        for copy in loads[1:]:
            copy.start()
        step_rows = 16

        def norm(i, carry):
            span = pl.ds(pl.multiple_of(i * step_rows, step_rows), step_rows)
            x = moe_v[span, :].astype(f32)
            level = lax.rsqrt(jnp.mean(x * x, axis=-1, keepdims=True) + EPSILON)
            normed[span, :] = (x * level * mgain_ref[...]).astype(bf16)
            return carry

        lax.fori_loop(0, row_count // step_rows, norm, 0, unroll=4)


    def direct(i, dx):
        return i == 0

    sent = {}

    def gather(i, dx):
        n = i * nx + dx
        if direct(i, dx):
            for o in range(n_y):
                out_x[n, o] = rows_for(at(i, dx), lane_block(o * CORES + my_c))
        else:
            out_z[n] = rows_for(at(i, dx), lane_block(tp))

    def send(i, dx):
        n = i * nx + dx
        if direct(i, dx):
            sent[n] = [
                to(
                    out_x.at[n, o],
                    g_moe.at[o * CORES + my_c, seen(dx)],
                    moe_x,
                    (dx - 1, o),
                    at(i, dx),
                    tp,
                    (nx - dx - 1, o),
                )
                for o in range(n_y)
            ]
        else:
            sent[n] = [
                to(out_z.at[n], g_moe.at[tp, seen(dx)], moe_a, (n,), at(i, dx), tp, (seen(dx),))
            ]

    def gone(i, dx):
        for copy in sent[i * nx + dx]:
            copy.wait_send()
            sends[:] = [other for other in sends if other is not copy]

    side = range(1, nx)
    wave = [(0, dx) for dx in side] + [(i, 0) for i in range(1, min(3, nz))]
    later = [(i, dx) for i in (2, 1) for dx in side if i < nz]
    latest = [(i, dx) for i in range(3, nz) for dx in range(nx)]
    with S("gather_a"):
        for pair in wave[:2]:
            gather(*pair)
    with S("barrier"):
        pl.semaphore_wait(barrier, n_ep + n_tp - 2)
    for pair in wave[:2]:
        send(*pair)
    with S("gather_b"):
        for pair in wave[2:]:
            gather(*pair)
            send(*pair)
    with S("gather_own"):
        for t in range(n_tp):
            g_moe[t, slot(0, 0)] = rows_for(me, slice(t * columns, (t + 1) * columns))
    with S("gather_c"):
        for pair in later:
            gather(*pair)
            send(*pair)
        for pair in latest:
            gather(*pair)

    with S("prep"):
        half = ROPE // 2
        pos = (me * row_count + lax.broadcasted_iota(jnp.int32, (half, row_count), 1)).astype(f32)
        band = lax.broadcasted_iota(jnp.int32, (half, row_count), 0)
        frequency = jnp.zeros((half, row_count), f32)
        for i in range(half):
            frequency = jnp.where(band == i, float(np.float32(frequency_of[i])), frequency)
        angle = pos * frequency
        cosine, sine = jnp.cos(angle), jnp.sin(angle)
        zero = lambda n: jnp.zeros((n, row_count), f32)
        rest = LANES - PLAIN_HEAD_DIM - ROPE
        cos_t = jnp.concatenate(
            [jnp.ones((PLAIN_HEAD_DIM, row_count), f32), cosine, cosine, zero(rest)], axis=0
        ).T
        down_t = jnp.concatenate([zero(PLAIN_HEAD_DIM), -sine, zero(half + rest)], axis=0).T
        up_t = jnp.concatenate([zero(PLAIN_HEAD_DIM + half), sine, zero(rest)], axis=0).T
        shared = rope_ref[...].astype(f32)
        first_half, second_half = shared[:half], shared[half:]
        rope_v[...] = jnp.concatenate(
            [
                zero(PLAIN_HEAD_DIM),
                first_half * cosine - second_half * sine,
                second_half * cosine + first_half * sine,
                zero(rest),
            ],
            axis=0,
        )
        own_lat = my_c * nx
        loads[1].wait()
        c = ckv_v[...].astype(f32)
        level = lax.rsqrt(jnp.mean(c * c, axis=-1, keepdims=True) + EPSILON)
        own_block = g_lat.at[own_lat, my_z]
        own_block[:, :latent] = (c * level * lgain_ref[...]).astype(bf16)
        own_block[:, latent:] = rope_v[:, half_rows].T.astype(bf16)
        loads[2].wait()
        width = PLAIN_HEAD_DIM + ROPE
        for h in range(heads):
            start = (h * width) // LANES * LANES
            shift = h * width - start
            size = LANES if shift + width <= LANES else 2 * LANES
            x = qraw[:, start : start + size].astype(f32)
            if shift:
                x = pltpu.roll(x, size - shift, 1)
            x = x[:, :LANES]
            q_ref[:, h * LANES : (h + 1) * LANES] = (
                x * cos_t + pltpu.roll(x, LANES - half, 1) * down_t + pltpu.roll(x, half, 1) * up_t
            ).astype(bf16)

    lat_over, lat_side = {}, {}

    def hop(block, way, z, ep_id, tp_id=tp):
        return pltpu.make_async_remote_copy(
            src_ref=block,
            dst_ref=block,
            send_sem=lat_z.at[way, z],
            recv_sem=lat_z.at[0, z],
            device_id=(ep_id, tp_id),
            device_id_type=pl.DeviceIdType.MESH,
        )

    def lat_hop(d):
        if d == 0:
            src = g_lat.at[own_lat, my_z]

            @pl.when(my_z + 1 < nz)
            def _():
                hop(src, 1, my_z, me + nx).start()

            @pl.when(my_z > 0)
            def _():
                hop(src, 2, my_z, me - nx).start()

            lat_share(my_z)
        else:
            @pl.when(my_z >= d)
            def _():
                z = my_z - d
                src = g_lat.at[own_lat, z]
                hop(src, 1, z, me, mate).wait_recv()

                @pl.when(my_z + 1 < nz)
                def _():
                    hop(src, 1, z, me + nx).start()

                lat_share(z)

            @pl.when(my_z + d < nz)
            def _():
                z = my_z + d
                src = g_lat.at[own_lat, z]
                hop(src, 2, z, me, mate).wait_recv()

                @pl.when(my_z > 0)
                def _():
                    hop(src, 2, z, me - nx).start()

                lat_share(z)

    def lat_share(z):
        mine = g_lat.at[own_lat, z]
        remote(mine, mine, lat_c, (0, z), (0, z), me, mate).start()
        if nx > 1:
            side = g_lat.at[own_lat + 1, z]
            remote(mine, side, lat_x, (z,), (z,), my_z * nx + 1 - my_x, tp).start()

    def lat_cross(z):
        if nx > 1:
            side = g_lat.at[own_lat + 1, z]
            come(side, lat_x, (z,))
            remote(side, side, lat_c, (1, z), (1, z), me, mate).start()

    def lat_done(z):
        for i in range(nx):
            come(g_lat.at[(1 - my_c) * nx + i, z], lat_c, (i, z))

    def lat_drain():
        for z in range(nz):
            block = g_lat.at[own_lat, z]

            @pl.when(jnp.logical_and(my_z >= z, my_z + 1 < nz))
            def _():
                hop(block, 1, z, me, mate).wait_send()

            @pl.when(jnp.logical_and(my_z <= z, my_z > 0))
            def _():
                hop(block, 2, z, me, mate).wait_send()

            remote(block, block, lat_c, (0, z), (0, z), me, mate).wait_send()
            if nx > 1:
                side = g_lat.at[own_lat + 1, z]
                remote(block, block, lat_x, (z,), (z,), me, mate).wait_send()
                remote(side, side, lat_c, (1, z), (1, z), me, mate).wait_send()

    relay_y, relay_c = {}, {}

    def arrive(i, dx):
        relay_c[i, dx] = []
        for o in range(n_y):
            block = g_moe.at[o * CORES + my_c, slot(i, dx)]
            come(block, moe_x, (dx - 1, o))
            relay_c[i, dx].append(to(block, block, moe_xc, (dx - 1, o), me, mate))

    def spread(i, dx, when=None):
        n = i * nx + dx
        block = g_moe.at[tp, slot(i, dx)]
        copies = []
        for o in range(1, n_y):
            other = lax.rem(my_y + o, n_y) * CORES + my_c
            relay_y[n, o] = remote(block, block, moe_y, (o - 1, n - nx), (o - 1, n - nx), me, other)
            copies.append(relay_y[n, o])
        relay_c[i, dx] = [remote(block, block, moe_c, (0, n - nx), (0, n - nx), me, mate)]
        copies += relay_c[i, dx]

        def run():
            come(block, moe_a, (slot(i, dx),))
            for copy in copies:
                copy.start()

        if when is None:
            run()
            sends.extend(copies)
        else:
            pl.when(when)(run)
            if (i, dx) not in spread_once:
                spread_once.add((i, dx))
                sends.extend(copies)

    spread_once = set()
    inner = jnp.logical_and(my_z > 0, my_z + 1 < nz)
    outer = jnp.logical_not(inner)

    def forward(i, dx):
        n = i * nx + dx
        for o in range(1, n_y):
            relay_y[n, o].wait_recv()
            came = g_moe.at[lax.rem(my_y + n_y - o, n_y) * CORES + my_c, slot(i, dx)]
            relay_c[i, dx].append(to(came, came, moe_c, (o, n - nx), me, mate))

    def finish(i):
        for dx in range(nx):
            for copy in relay_c.get((i, dx), ()):
                copy.wait_recv()

    units = [(0, (dx,)) for dx in range(nx)] + [(c, tuple(range(nx))) for c in range(1, nz)]

    def up(u, f):
        c, dxs = units[u]
        span = slice(f * tile, (f + 1) * tile)
        rows = len(dxs) * cap
        gate = jnp.zeros((rows, tile), f32)
        lift = jnp.zeros((rows, tile), f32)
        for t in range(n_tp):
            x = merge_rows(g_moe[t, pl.ds(slot(c, dxs[0]), len(dxs))])
            gate += jnp.dot(
                x, wg[t * columns : (t + 1) * columns, span], preferred_element_type=f32
            )
            lift += jnp.dot(
                x, wu[t * columns : (t + 1) * columns, span], preferred_element_type=f32
            )
        hidden[:rows, span] = (gate / (1.0 + jnp.exp(-gate)) * lift).astype(bf16)

    reduce_c, reduce_y = {}, {}

    def down(u):
        c, dxs = units[u]
        n = c * nx + dxs[0]
        group = slice(n, n + len(dxs))
        span = pl.ds(n, len(dxs))
        for o in list(range(1, n_y)) + [0]:
            y = lax.rem(my_y + o, n_y)
            for mine in range(2):
                t = y * CORES + (my_c if mine else 1 - my_c)
                part[t, group] = (
                    jnp.dot(
                        hidden[: len(dxs) * cap],
                        wd[:, lane_block(t)],
                        preferred_element_type=f32,
                    )
                    .astype(bf16)
                    .reshape(len(dxs), cap, columns)
                )
                if not mine:
                    reduce_c[u, o] = to(part.at[t, span], r1.at[o, span], red_c, (o, u), me, mate)

    def level_two(u):
        c, dxs = units[u]
        for o in range(1, n_y):
            y = lax.rem(my_y + o, n_y)
            reduce_c[u, o].wait_recv()
            for dx in dxs:
                n = c * nx + dx
                s2[o, n] = (
                    part[y * CORES + my_c, n].astype(f32) + r1[o, n].astype(f32)
                ).astype(bf16)
                reduce_y[n, o] = to(
                    s2.at[o, n], r2.at[o, n], red_y, (o - 1, n), me, y * CORES + my_c
                )

    def give_back(u):
        c, dxs = units[u]
        reduce_c[u, 0].wait_recv()
        for dx in dxs:
            n = c * nx + dx
            total = part[tp, n].astype(f32) + r1[0, n].astype(f32)
            for o in range(1, n_y):
                reduce_y[n, o].wait_recv()
                total += r2[o, n].astype(f32)
            tot[n] = total.astype(bf16)
            if n > 0:
                to(tot.at[n], back.at[seen(dx)], ret_a, (n,), at(c, dx), tp, (seen(dx),))

    def combine(i, dx):
        if i == 0 and dx == 0:
            came = tot[0]
        else:
            come(back.at[slot(i, dx)], ret_a, (slot(i, dx),))
            came = back[slot(i, dx)]
        e = at(i, dx)
        weight = jnp.where(chosen(e), mix_ref[pl.ds(e, 1), :], 0.0)
        high = weight.astype(bf16)
        low = (weight - high.astype(f32)).astype(bf16)
        add = lax.dot_general(
            jnp.concatenate([high, low], axis=0),
            jnp.concatenate([came, came], axis=0),
            (((0,), (0,)), ((), ())),
            preferred_element_type=f32,
        )
        if i == 0 and dx == 0:
            acc[...] = add
        else:
            acc[...] += add

    block = nz * share

    def expand(z):
        lat_done(z)
        for t in range(g_lat.shape[0]):
            span = pl.ds(pl.multiple_of(t * block + z * share, share), share)
            kv[span, :] = jnp.dot(
                g_lat[t, z][:, :latent], wkv_ref[...], preferred_element_type=f32
            ).astype(bf16)

    def around(d, f):
        if d == 0:
            f(my_z)
        else:
            pl.when(my_z >= d)(lambda: f(my_z - d))
            pl.when(my_z + d < nz)(lambda: f(my_z + d))

    whole_lat = g_lat.reshape(g_lat.shape[0] * block, g_lat.shape[3])
    lane = lax.broadcasted_iota(jnp.int32, (1, LANES), 1)
    packed = 2 if heads % 2 == 0 else 1
    parts = heads // packed
    att_in, att_mate = [], []

    def attend(part_index):
        for h in range(part_index * packed, (part_index + 1) * packed):
            head = kv[:, h * LANES : (h + 1) * LANES]
            keys = jnp.where(lane < PLAIN_HEAD_DIM, head, whole_lat[:, latent : latent + LANES])
            scores = (
                lax.dot_general(
                    q_ref[:, h * LANES : (h + 1) * LANES],
                    keys,
                    (((1,), (1,)), ((), ())),
                    preferred_element_type=f32,
                )
                * scale
            )
            peak = jnp.max(scores, axis=-1, keepdims=True)
            e = jnp.exp(scores - peak)
            total = jnp.sum(e, axis=-1, keepdims=True)
            mixed = jnp.dot(e.astype(bf16), head, preferred_element_type=f32) / total
            if packed == 1:
                mixed = jnp.where(lane < PLAIN_HEAD_DIM, 0.0, mixed)
            elif h % 2 == 0:
                held = pltpu.roll(mixed, VALUE_HEAD_DIM, 1)
            else:
                mixed = jnp.where(lane < VALUE_HEAD_DIM, held, mixed)
        g_att[tp, part_index] = mixed.astype(bf16)

    def att_send(p):
        own = g_att.at[tp, p]
        for o in range(1, n_y):
            other = lax.rem(my_y + o, n_y) * CORES + my_c
            att_in.append((p, o, to(own, own, att_y, (o - 1, p), me, other)))
        att_mate.append(to(own, own, att_c, (0, p), me, mate))

    def att_forward(part_index):
        for p, o, copy in att_in:
            if p == part_index:
                copy.wait_recv()
                came = g_att.at[lax.rem(my_y + n_y - o, n_y) * CORES + my_c, p]
                att_mate.append(to(came, came, att_c, (o, p), me, mate))

    att_copy = pltpu.make_async_copy(att_v, att_dst, in_sem.at[13])
    exp_copy = pltpu.make_async_copy(exp_v, exp_dst, in_sem.at[14])

    def project():
        for copy in att_mate:
            copy.wait_recv()
        total = jnp.zeros(att_v.shape, f32)
        for t in range(n_tp):
            x = jnp.concatenate([g_att[t, p] for p in range(g_att.shape[1])], axis=1)
            width = x.shape[1]
            total += jnp.dot(x, wo_ref[t * width : (t + 1) * width, :], preferred_element_type=f32)
        att_v[...] = total.astype(bf16)
        att_copy.start()

    def weights_in():
        for copy in loads[3:]:
            copy.wait()

    def each(name, f, i, some=range(nx)):
        for dx in some:
            scoped("%s%d%d" % (name, i, dx), f, i, dx)

    def half_up(u, k):
        with S("up%d_%d" % (u, k)):
            for f in range(tiles):
                if (2 * f) // tiles == k:
                    up(u, f)

    last = nz - 1
    first = nx - 1
    scoped("weights", weights_in)
    for pair in latest:
        send(*pair)
    half_up(0, 0)
    if nz > 1:
        each("spread", spread, 1, range(1))
    half_up(0, 1)
    scoped("down0", down, 0)
    each("arrive", arrive, 0, side)
    scoped("level_two0", level_two, 0)
    scoped("finish0", finish, 0)
    for u in range(1, nx):
        half_up(u, 0)
        if nz > 1 and u == 1:
            for dx in side:
                scoped("ospread1%d" % dx, spread, 1, dx, outer)
        half_up(u, 1)
        scoped("down%d" % u, down, u)
    if nz > 1:
        for dx in side:
            scoped("ispread1%d" % dx, spread, 1, dx, inner)
    if nz > 2:
        scoped("ispread20", spread, 2, 0, inner)
    if nz > 1:
        each("forward", forward, 1, range(1))
    for u in range(1, nx):
        scoped("level_two%d" % u, level_two, u)
    scoped("lat0", lat_hop, 0)
    if nz > 2:
        for dx in side:
            scoped("ispread2%d" % dx, spread, 2, dx, inner)
    if nz > 1:
        each("forward", forward, 1, side)
        scoped("finish1", finish, 1)
        half_up(first + 1, 0)
    if nz > 2:
        for dx in range(nx):
            scoped("ospread2%d" % dx, spread, 2, dx, outer)
    for i in range(3, nz):
        each("spread", spread, i)
    if nz > 1:
        half_up(first + 1, 1)
        scoped("down%d" % (first + 1), down, first + 1)
        scoped("lat1", lat_hop, 1)
        if nz > 2:
            each("forward", forward, 2)
    for c in range(2, nz):
        u = first + c
        scoped("finish%d" % c, finish, c)
        scoped("level_two%d" % (u - 1), level_two, u - 1)
        half_up(u, 0)
        if c + 1 < nz:
            each("forward", forward, c + 1, range(1))
        if c == 2:
            for v in range(nx):
                scoped("give_back%d" % v, give_back, v)
        else:
            scoped("give_back%d" % (u - 2), give_back, u - 2)
        scoped("lat%d" % c, lat_hop, c)
        half_up(u, 1)
        if c + 1 < nz:
            each("forward", forward, c + 1, side)
        scoped("down%d" % u, down, u)
    final = len(units) - 1
    scoped("level_two%d" % final, level_two, final)
    if nz > 1:
        scoped("give_back%d" % (final - 1), give_back, final - 1)
    if nz == 2:
        for v in range(nx):
            scoped("give_back%d" % v, give_back, v)
    for d in range(min(2, nz)):
        scoped("cross%d" % d, around, d, lat_cross)
    scoped("expand0", around, 0, expand)
    for d in range(2, nz):
        if d == last:
            scoped("expand%d" % (d - 2), around, d - 2, expand)
            scoped("expand%d" % (d - 1), around, d - 1, expand)
            scoped("cross%d" % d, around, d, lat_cross)
        else:
            scoped("cross%d" % d, around, d, lat_cross)
            if d > 2:
                scoped("expand%d" % (d - 2), around, d - 2, expand)
    each("combine", combine, 0)
    scoped("give_back%d" % final, give_back, final)
    if nz > 1:
        scoped("expand%d" % last, around, last, expand)
    for p in range(parts):
        scoped("attend%d" % p, attend, p)
        att_send(p)
    for p in range(parts):
        scoped("att_forward%d" % p, att_forward, p)
    scoped("project", project)
    for i in range(1, nz):
        each("combine", combine, i)
    exp_v[...] = acc[...].astype(bf16)
    exp_copy.start()
    with S("sendwait"):
        for copy in sends:
            copy.wait_send()
    with S("latdrain"):
        lat_drain()
    with S("outwait"):
        att_copy.wait()
        exp_copy.wait()


def local(
    queries,
    compressed_key_value,
    rope_key,
    latent_norm_gain,
    latent_to_key_value,
    out_proj,
    moe_input,
    moe_gain,
    routes,
    route_weight,
    gate_weight,
    up_weight,
    down_weight,
):
    n_ep = lax.axis_size("ep")
    n_tp = lax.axis_size("tp")
    n_y = n_tp // CORES
    bf16 = jnp.bfloat16
    row_count = queries.shape[0]
    heads = latent_to_key_value.shape[1] // (PLAIN_HEAD_DIM + VALUE_HEAD_DIM)
    latent = compressed_key_value.shape[1]
    share = row_count // CORES
    nx, nz = ep_shape(n_ep)
    over = -queries.shape[1] % LANES
    if over:
        queries = jnp.pad(queries, ((0, 0), (0, over)))
    if heads % 2 == 0:
        wo = out_proj
        parts = heads // 2
    else:
        wo = out_proj.reshape(n_tp * heads, VALUE_HEAD_DIM, out_proj.shape[1])
        wo = jnp.concatenate([jnp.zeros_like(wo), wo], axis=1)
        wo = wo.reshape(n_tp * heads * LANES, out_proj.shape[1])
        parts = heads
    model_width = moe_input.shape[1]
    top = routes.shape[1]
    capacity = 3 * row_count // n_ep
    places = -(-capacity // 16) * 16
    columns = model_width // n_tp
    ff = gate_weight.shape[2]
    anywhere = pl.BlockSpec(memory_space=pl.ANY)
    hbm = pl.BlockSpec(memory_space=pltpu.HBM)
    dma = lambda *shape: pltpu.SemaphoreType.DMA((2,) + shape)
    attention, experts = pl.pallas_call(
        functools.partial(fused, n_ep, n_tp, heads, (PLAIN_HEAD_DIM + ROPE) ** (-0.5)),
        out_shape=(
            pltpu.VMEM((row_count, out_proj.shape[1]), bf16),
            pltpu.VMEM((row_count, columns), bf16),
        ),
        in_specs=[hbm] * 13,
        out_specs=(anywhere, anywhere),
        scratch_shapes=[
            pltpu.VMEM((top, row_count), jnp.int32),
            pltpu.VMEM((top, row_count), jnp.float32),
            pltpu.VMEM((1, model_width), jnp.float32),
            pltpu.VMEM((1, latent), jnp.float32),
            pltpu.VMEM((ROPE, row_count), bf16),
            pltpu.VMEM((row_count, model_width), bf16),
            pltpu.VMEM((share, latent), bf16),
            pltpu.VMEM(queries.shape, bf16),
            pltpu.VMEM(latent_to_key_value.shape, bf16),
            pltpu.VMEM(wo.shape, bf16),
            pltpu.VMEM((model_width, ff), bf16),
            pltpu.VMEM((model_width, ff), bf16),
            pltpu.VMEM((ff, model_width), bf16),
            pltpu.VMEM((row_count, model_width), bf16),
            pltpu.VMEM((n_ep, row_count), jnp.int32),
            pltpu.VMEM((n_ep, row_count), jnp.float32),
            pltpu.VMEM((n_ep, places, columns), bf16),
            pltpu.VMEM((nx, n_y, places, columns), bf16),
            pltpu.VMEM((LANES, row_count), jnp.float32),
            pltpu.VMEM((row_count, heads * LANES), bf16),
            pltpu.VMEM((CORES * nx, nz, share, latent + LANES), bf16),
            pltpu.VMEM((n_tp, n_ep, places, columns), bf16),
            pltpu.VMEM((n_tp, parts, row_count, LANES), bf16),
            pltpu.VMEM((n_ep * row_count, heads * LANES), bf16),
            pltpu.VMEM((nx * places, ff), bf16),
            pltpu.VMEM((n_tp, n_ep, places, columns), bf16),
            pltpu.VMEM((n_y, n_ep, places, columns), bf16),
            pltpu.VMEM((n_y, n_ep, places, columns), bf16),
            pltpu.VMEM((n_y, n_ep, places, columns), bf16),
            pltpu.VMEM((n_ep, places, columns), bf16),
            pltpu.VMEM((n_ep, places, columns), bf16),
            pltpu.VMEM((row_count, columns), jnp.float32),
            pltpu.VMEM((row_count, out_proj.shape[1]), bf16),
            pltpu.VMEM((row_count, columns), bf16),
            pltpu.SemaphoreType.DMA((15,)),
            pltpu.SemaphoreType.DMA((3, nz)),
            dma(nz),
            dma(nx, nz),
            dma(n_ep),
            dma(max(nx - 1, 1), n_y),
            dma(max(nx - 1, 1), n_y),
            dma(max(n_y - 1, 1), max(n_ep - nx, 1)),
            dma(n_y, max(n_ep - nx, 1)),
            dma(max(n_y - 1, 1), parts),
            dma(n_y, parts),
            dma(n_y, nx + nz - 1),
            dma(max(n_y - 1, 1), n_ep),
            dma(n_ep),
        ],
        compiler_params=pltpu.CompilerParams(
            collective_id=0, has_side_effects=True, vmem_limit_bytes=60 * 1024 * 1024
        ),
        name="fused",
    )(
        routes.T,
        route_weight.T,
        moe_gain.reshape(1, model_width),
        latent_norm_gain.reshape(1, latent),
        rope_key.T,
        moe_input,
        compressed_key_value,
        queries,
        latent_to_key_value,
        wo,
        gate_weight.reshape(model_width, ff),
        up_weight.reshape(model_width, ff),
        down_weight.reshape(ff, model_width),
    )
    return attention, experts


def solution(mesh):
    return jax.shard_map(
        local,
        mesh=mesh,
        in_specs=(
            P("ep", "tp"),
            P("ep", None),
            P("ep", None),
            P(),
            P(None, "tp"),
            P(None, "tp"),
            P("ep", None),
            P(),
            P("ep", None),
            P("ep", None),
            P("ep", None, "tp"),
            P("ep", None, "tp"),
            P("ep", "tp", None),
        ),
        out_specs=(P("ep", "tp"), P("ep", "tp")),
        check_vma=False,
    )
```
